32 devices in a mesh: kv: 16 (over z, y, core), tp: 2 (over x).
Axes of the slice: x: 2, y: 2, z: 4, core: 2. Of those that a mesh axis runs over, the one named last changes fastest.
Arguments:
- hidden_rows: bfloat16 [6144, 2048], P('kv'), may hold values from -6 to 6
- proj_query: bfloat16 [2048, 2048], P(None, 'tp'), may hold values from -0.125 to 0.125
- proj_key: bfloat16 [2048, 256], P(None, 'tp'), may hold values from -0.125 to 0.125
- proj_value: bfloat16 [2048, 256], P(None, 'tp'), may hold values from -0.125 to 0.125
- proj_output: bfloat16 [2048, 2048], P('tp'), may hold values from -0.125 to 0.125
- head_scale: float32 [32], P('tp'), may hold values from 0.25 to 96
- hot_blocks: int32 [16], replicated, may hold values from 0 to 191, as said below
- chosen_blocks: int32 [96, 16], P('kv'), may hold values from 0 to 27, as said below
Outputs:
- layer_out: bfloat16 [6144, 2048], P('kv', 'tp')
The draws below stay inside these ranges and needn't reach their ends.
Inputs may be any that keep to these rules, and one draw needn't show every extreme that they name: `hot_blocks`: 16 different key-block numbers; no device's 12 key blocks hold more than 2 of them, and in every draw some device holds exactly 2. `chosen_blocks`: each row's 16 codes name different key blocks; among them are the key blocks that cover the positions of query block b; no code of 12 or more names a block on the query block's own device.
All inputs are finite; a program needn't handle non-finite values.
Results may differ from the reference program's by a relative error of at most 0.01.
The reference program's roundings to bfloat16 on the way count: a program that leaves them out, or rounds other values in their place, can miss the bound.
Values may be sent and summed in bfloat16 or wider, within the bound.
A program may use at most 64 MiB of HBM per device.

```python
import math
import jax
import jax.numpy as jnp
from jax import lax

D = 2048
H = 32
HD = 64
KVH = 4
KB = 32
QB = 64
NSEL = 16
NHOT = 16
TOK_DEV = 384
SEQ = 6144
NQB = 96
NKB = 192
KB_DEV = 12
N_KV = 16
N_TP = 2


def make_hot(key):
    base = jax.random.fold_in(key, 7001)
    key_perm, key_block, key_step, key_order = jax.random.split(base, 4)
    owners = jax.random.permutation(key_perm, N_KV).astype(jnp.int32)
    leader = owners[0]
    opposite = (leader + N_KV // 2) % N_KV
    remaining = owners[1:]
    order = jnp.argsort((remaining == opposite).astype(jnp.int32), stable=True)
    others = remaining[order][:NHOT - 3]
    owner_list = jnp.concatenate([jnp.stack([leader, leader, opposite]), others])
    blocks = jax.random.randint(key_block, (NHOT,), 0, KB_DEV, dtype=jnp.int32)
    offset_step = jax.random.randint(key_step, (), 1, KB_DEV, dtype=jnp.int32)
    blocks = blocks.at[1].set((blocks[0] + offset_step) % KB_DEV)
    block_ids = owner_list * KB_DEV + blocks
    return block_ids[jax.random.permutation(key_order, NHOT)].astype(jnp.int32)


def draw_hot_blocks(key, part):
    return make_hot(key)


def draw_chosen_blocks(key, part):
    hot = make_hot(key)
    per_block = QB // KB
    count = KB_DEV + NHOT
    qblock = jnp.arange(NQB, dtype=jnp.int32)
    device = qblock // (TOK_DEV // QB)
    local_ids = device[:, None] * KB_DEV + jnp.arange(KB_DEV, dtype=jnp.int32)[None, :]
    candidates = jnp.concatenate([local_ids, jnp.broadcast_to(hot[None, :], (NQB, NHOT))], axis=1)
    noise = jax.random.randint(jax.random.fold_in(key, 7002), (NQB, count), 0, 1000, dtype=jnp.int32)
    first_own = qblock * per_block
    own_cover = (candidates >= first_own[:, None]) & (candidates < first_own[:, None] + per_block)
    earlier = candidates < first_own[:, None] + per_block
    duplicate = (jnp.arange(count, dtype=jnp.int32)[None, :] >= KB_DEV) & (candidates // KB_DEV == device[:, None])
    score = noise + 10000 * earlier.astype(jnp.int32) + 100000 * own_cover.astype(jnp.int32)
    score = score - 1000000 * duplicate.astype(jnp.int32)
    score = score * count + jnp.arange(count, dtype=jnp.int32)[None, :]
    _, picked = lax.top_k(score, NSEL)
    return picked.astype(jnp.int32)


def draw_head_scale(key, part):
    key_low = jax.random.fold_in(jax.random.fold_in(key, 7003), 1)
    return jnp.exp(jax.random.uniform(key_low, (H,), jnp.float32, math.log(0.5), math.log(4.0)))


def levels(own_key, shape, cuts, low, high):
    level, own = 1.0, jax.random.fold_in(own_key, 6)
    for axis_at, parts in cuts:
        heights = jnp.exp(jax.random.uniform(jax.random.fold_in(own, axis_at), (parts,), jnp.float32, low / len(cuts), high / len(cuts)))
        level = level * jnp.repeat(heights, shape[axis_at] // parts).reshape([-1 if axis == axis_at else 1 for axis in range(len(shape))])
    return level


def gaussian(own_key, extent, deviation, limit, pieces=(), held_as=jnp.bfloat16):
    array = jax.random.normal(own_key, extent, jnp.float32) * deviation
    if len(pieces) > 0:
        array = levels(own_key, extent, pieces, -0.22, 0.18) * array
    return jnp.clip(array, min=-limit, max=limit).astype(held_as)


def setup_inputs(seed: int = 0) -> dict:
    splits = jax.random.split(jax.random.key(seed), 9)
    return {
        "hidden_rows": gaussian(splits[0], (SEQ, D), 1.0, 6.0, ((0, 16),)),
        "proj_query": gaussian(splits[1], (D, H * HD), D ** -0.5, 0.125, ((1, 2),)),
        "proj_key": gaussian(splits[2], (D, KVH * HD), D ** -0.5, 0.125, ((1, 2),)),
        "proj_value": gaussian(splits[3], (D, KVH * HD), D ** -0.5, 0.125, ((1, 2),)),
        "proj_output": gaussian(splits[4], (H * HD, D), (H * HD) ** -0.5, 0.125, ((0, 2),)),
        "head_scale": draw_head_scale(jax.random.fold_in(splits[8], 71), 0),
        "hot_blocks": draw_hot_blocks(jax.random.fold_in(splits[8], 71), 0),
        "chosen_blocks": draw_chosen_blocks(jax.random.fold_in(splits[8], 71), 0),
    }


def reference(hidden_rows, proj_query, proj_key, proj_value, proj_output, head_scale, hot_blocks, chosen_blocks):
    group_size = H // KVH
    per_device = TOK_DEV // QB
    queries = jnp.dot(hidden_rows, proj_query, preferred_element_type=jnp.float32).astype(jnp.bfloat16)
    key_proj = jnp.dot(hidden_rows, proj_key, preferred_element_type=jnp.float32).astype(jnp.bfloat16)
    value_proj = jnp.dot(hidden_rows, proj_value, preferred_element_type=jnp.float32).astype(jnp.bfloat16)
    queries = queries.reshape(NQB, QB, KVH, group_size, HD)
    key_proj = key_proj.reshape(NKB, KB, KVH, HD)
    value_proj = value_proj.reshape(NKB, KB, KVH, HD)
    scale_grid = head_scale.reshape(KVH, group_size)

    def attend(block_index):
        codes = chosen_blocks[block_index]
        holder = (block_index // per_device).astype(jnp.int32)
        hot_index = jnp.clip(codes - KB_DEV, 0, NHOT - 1).astype(jnp.int32)
        picked = jnp.where(codes < KB_DEV, holder * KB_DEV + codes, hot_blocks[hot_index]).astype(jnp.int32)
        key_rows = key_proj[picked].reshape(NSEL * KB, KVH, HD).astype(jnp.float32)
        value_rows = value_proj[picked].reshape(NSEL * KB, KVH, HD).astype(jnp.float32)
        query_rows = queries[block_index].astype(jnp.float32)
        scores = jnp.einsum('qcgd,lcd->cgql', query_rows, key_rows) * (HD ** -0.5)
        scores = scores * scale_grid[:, :, None, None]
        query_pos = block_index * QB + jnp.arange(QB, dtype=jnp.int32)
        key_pos = (picked[:, None] * KB + jnp.arange(KB, dtype=jnp.int32)[None, :]).reshape(NSEL * KB)
        visible = key_pos[None, :] <= query_pos[:, None]
        scores = jnp.where(visible[None, None], scores, -jnp.inf)
        row_max = jnp.max(scores, axis=-1, keepdims=True)
        lifted = jnp.exp(scores - row_max)
        weights = lifted / jnp.sum(lifted, axis=-1, keepdims=True)
        weights = lax.optimization_barrier(weights.astype(jnp.bfloat16)).astype(jnp.float32)
        attended = jnp.einsum('cgql,lcd->qcgd', weights, value_rows)
        return attended.reshape(QB, H * HD).astype(jnp.bfloat16)

    heads_out = lax.map(attend, jnp.arange(NQB, dtype=jnp.int32)).reshape(NQB * QB, H * HD)
    width = H * HD // N_TP
    total = jnp.zeros((NQB * QB, D), jnp.float32)
    for group_index in range(N_TP):
        begin = group_index * width
        partial_value = jnp.dot(heads_out[:, begin:begin + width], proj_output[begin:begin + width],
                          preferred_element_type=jnp.float32)
        total = total + lax.optimization_barrier(partial_value.astype(jnp.bfloat16)).astype(jnp.float32)
    return total.astype(jnp.bfloat16)
```

```python
import functools

import jax
import jax.numpy as jnp
from jax import lax
from jax.experimental import pallas as pl
from jax.experimental.pallas import tpu as pltpu
from jax.sharding import PartitionSpec as P

HD = 64
KB = 32
QB = 64
HOT_MOST = 2
LANES = 128
PIECES = 4
LOG2E = 1.4426950408889634
MESH = pl.DeviceIdType.MESH


def dot(a, b):
    return jnp.dot(a, b, preferred_element_type=jnp.float32)


def kernel(
    n,
    n_tp,
    x_hbm,
    wq_hbm,
    wk_hbm,
    wv_hbm,
    wo_hbm,
    scale_hbm,
    hot_hbm,
    chosen_hbm,
    out,
    x,
    wq,
    wk,
    wv,
    wo,
    q,
    local,
    pool,
    kvg,
    heads,
    sent,
    got,
    mine_part,
    bias,
    scale_ref,
    hot_ref,
    chosen_ref,
    slot_ref,
    small_sem,
    load_sem,
    wq_sem,
    wo_sem,
    hot_send,
    pass_send,
    hot_recv,
    part_send,
    part_recv,
):
    me = lax.axis_index("kv")
    t = lax.axis_index("tp")
    own = local.shape[0]
    width = local.shape[2]
    nsel = chosen_ref.shape[1]
    nhot = hot_ref.shape[0]
    blocks = chosen_ref.shape[0]
    head_count = scale_ref.shape[0]
    kv_heads = wk.shape[1] // HD
    pairs = head_count // kv_heads // 2
    keys = nsel * KB
    part_cols = wo.shape[2]
    partner = me + 1 - 2 * lax.rem(me, 2)
    half = n // 2

    depth = x.shape[1] // PIECES
    cuts = [slice(i * depth, (i + 1) * depth) for i in range(PIECES)]
    loads = [
        [
            pltpu.make_async_copy(x_hbm.at[:, cut], x.at[:, cut], load_sem.at[3 * i]),
            pltpu.make_async_copy(wk_hbm.at[cut], wk.at[cut], load_sem.at[3 * i + 1]),
            pltpu.make_async_copy(wv_hbm.at[cut], wv.at[cut], load_sem.at[3 * i + 2]),
        ]
        for i, cut in enumerate(cuts)
    ]
    smalls = [
        pltpu.make_async_copy(hot_hbm, hot_ref, small_sem.at[0]),
        pltpu.make_async_copy(chosen_hbm, chosen_ref, small_sem.at[1]),
        pltpu.make_async_copy(scale_hbm, scale_ref, small_sem.at[2]),
    ]
    for load in loads[0]:
        load.start()
    for small in smalls:
        small.start()
    for piece in loads[1:]:
        for load in piece:
            load.start()
    q_chunk = wq.shape[2]
    wq_loads = [
        pltpu.make_async_copy(wq_hbm.at[:, pl.ds(i * q_chunk, q_chunk)], wq.at[i], wq_sem.at[i])
        for i in range(wq.shape[0])
    ]
    targets = [lax.rem(t + k, n_tp) for k in range(n_tp)]
    order = list(range(1, n_tp)) + [0]
    wo_loads = [
        pltpu.make_async_copy(
            wo_hbm.at[:, pl.ds(pl.multiple_of(targets[k] * part_cols, LANES), part_cols)],
            wo.at[k],
            wo_sem.at[k],
        )
        for k in range(n_tp)
    ]

    barrier = pltpu.get_barrier_semaphore()

    def greet(j, carry):
        pl.semaphore_signal(
            barrier, inc=1, device_id=(lax.rem(me + 2 * j, n), t), device_id_type=MESH
        )
        return carry

    lax.fori_loop(1, half, greet, 0)
    pl.semaphore_signal(barrier, inc=1, device_id=(partner, t), device_id_type=MESH)
    for k in range(1, n_tp):
        pl.semaphore_signal(barrier, inc=1, device_id=(me, targets[k]), device_id_type=MESH)

    for small in smalls:
        small.wait()
    hots = [hot_ref[h] for h in range(nhot)]
    owners = [lax.div(hot, own) for hot in hots]
    mine = [jnp.int32(0), jnp.int32(0)]
    for h in range(nhot):
        rank = jnp.int32(0)
        for g in range(h):
            rank = rank + (owners[g] == owners[h]).astype(jnp.int32)
        slot_ref[h] = own + owners[h] * HOT_MOST + rank
        offset = hots[h] - owners[h] * own
        for r in range(HOT_MOST):
            mine[r] = jnp.where((owners[h] == me) & (rank == r), offset, mine[r])

    total = None
    for piece, cut in zip(loads, cuts):
        for load in piece:
            load.wait()
        if total is None:
            for load in wq_loads:
                load.start()
            for k in order:
                wo_loads[k].start()
        term = dot(x[:, cut], jnp.concatenate([wk[cut], wv[cut]], axis=1))
        total = term if total is None else total + term
    packed = total.astype(jnp.bfloat16).reshape(own, KB, width)
    local[...] = packed
    pool[pl.ds(0, own)] = packed
    first = own + me * HOT_MOST
    for r in range(HOT_MOST):
        pool[first + r] = local[mine[r]]
    pl.semaphore_wait(barrier, half + n_tp - 1)

    def give(source, device, send):
        rows = pl.ds(own + source * HOT_MOST, HOT_MOST)
        return pltpu.make_async_remote_copy(
            src_ref=pool.at[rows],
            dst_ref=pool.at[rows],
            send_sem=send,
            recv_sem=hot_recv.at[source],
            device_id=(device, t),
            device_id_type=MESH,
        )

    def send_own(j, carry):
        give(me, lax.rem(me + 2 * j, n), hot_send.at[j]).start()
        return carry

    lax.fori_loop(1, half, send_own, 0)
    give(me, partner, hot_send.at[0]).start()

    for i in range(wq.shape[0]):
        wq_loads[i].wait()
        q[:, i * q_chunk : (i + 1) * q_chunk] = dot(x[...], wq[i]).astype(jnp.bfloat16)

    lane = lax.broadcasted_iota(jnp.int32, (1, keys), 1)
    in_block = lax.rem(lane, KB)
    entry_of = lax.div(lane, KB)

    def mask(b, carry):
        key_pos = in_block
        for e in range(nsel):
            code = chosen_ref[b, e]
            listed = jnp.clip(code - own, 0, nhot - 1)
            block_id = jnp.where(code < own, me * own + code, hot_ref[listed])
            key_pos = jnp.where(entry_of == e, block_id * KB + in_block, key_pos)
        query_pos = (me * blocks + b) * QB + lax.broadcasted_iota(jnp.int32, (QB, keys), 0)
        bias[b] = jnp.where(key_pos <= query_pos, 0.0, -jnp.inf).astype(jnp.float32)
        return carry

    lax.fori_loop(0, blocks, mask, 0)

    def pass_on(j, carry):
        source = lax.rem(me + n - 2 * j, n)
        copy = give(source, partner, pass_send.at[j])
        copy.wait_recv()
        copy.start()
        return carry

    lax.fori_loop(1, half, pass_on, 0)

    def land(j, carry):
        source = lax.rem(partner + n - 2 * j, n)
        give(source, partner, pass_send.at[0]).wait_recv()
        return carry

    lax.fori_loop(0, half, land, 0)
    for k in range(1, n_tp):
        wo_loads[k].wait()

    low = lax.broadcasted_iota(jnp.int32, (keys, LANES), 1) < HD
    zero = jnp.zeros((keys, LANES), jnp.bfloat16)
    ones = jnp.ones((keys, LANES), jnp.bfloat16)
    ones_low, ones_high = jnp.where(low, ones, zero), jnp.where(low, zero, ones)

    def part_copy(k, b):
        at = (k - 1) * blocks + b
        return pltpu.make_async_remote_copy(
            src_ref=sent.at[k - 1, b],
            dst_ref=got.at[k - 1, b],
            send_sem=part_send.at[at],
            recv_sem=part_recv.at[at],
            device_id=(me, targets[k]),
            device_id_type=MESH,
        )

    def attend(b, carry):
        for e in range(nsel):
            code = chosen_ref[b, e]
            listed = jnp.clip(code - own, 0, nhot - 1)
            row = jnp.where(code < own, code, slot_ref[listed])
            kvg[e * KB : (e + 1) * KB, :] = pool[row]
        rows = pl.ds(pl.multiple_of(b * QB, QB), QB)

        def spread(u):
            tile = kvg[:, (u // 2) * LANES : (u // 2 + 1) * LANES]
            turned = jnp.concatenate([tile[:, HD:], tile[:, :HD]], axis=1)
            if u % 2 == 1:
                tile, turned = turned, tile
            return jnp.where(low, tile, zero), jnp.where(low, zero, turned)

        for c in range(kv_heads):
            k_low, k_high = spread(c)
            k_both = jnp.concatenate([k_low, k_high], axis=0)
            v_low, v_high = spread(kv_heads + c)
            v_both = jnp.concatenate(
                [
                    jnp.concatenate([v_low, ones_low], axis=1),
                    jnp.concatenate([v_high, ones_high], axis=1),
                ],
                axis=0,
            )
            first_pair = c * pairs
            q_rows = jnp.concatenate(
                [
                    q[rows, (first_pair + p) * LANES : (first_pair + p + 1) * LANES]
                    for p in range(pairs)
                ],
                axis=0,
            )
            scores = lax.dot_general(
                q_rows, k_both, (((1,), (1,)), ((), ())), preferred_element_type=jnp.float32
            )
            lifted = []
            for p in range(pairs):
                both = []
                for s in range(2):
                    factor = scale_ref[(first_pair + p) * 2 + s] * (HD**-0.5 * LOG2E)
                    part = scores[p * QB : (p + 1) * QB, s * keys : (s + 1) * keys]
                    part = part * factor + bias[b]
                    top = jnp.max(part, axis=1, keepdims=True)
                    both.append(jnp.exp2(part - top).astype(jnp.bfloat16))
                lifted.append(jnp.concatenate(both, axis=1))
            summed = dot(jnp.concatenate(lifted, axis=0), v_both)
            held = (summed[:, :LANES] / summed[:, LANES:]).astype(jnp.bfloat16)
            for p in range(pairs):
                heads[rows, (first_pair + p) * LANES : (first_pair + p + 1) * LANES] = held[
                    p * QB : (p + 1) * QB
                ]
        for k in range(1, n_tp):
            sent[k - 1, b] = dot(heads[rows, :], wo[k]).astype(jnp.bfloat16)
            part_copy(k, b).start()
        return carry

    lax.fori_loop(0, blocks, attend, 0)

    wo_loads[0].wait()
    mine_part[...] = dot(heads[...], wo[0]).astype(jnp.bfloat16)

    def finish(b, carry):
        rows = pl.ds(pl.multiple_of(b * QB, QB), QB)
        total = mine_part[rows, :].astype(jnp.float32)
        for k in range(1, n_tp):
            part_copy(k, b).wait()
            total = total + got[k - 1, b].astype(jnp.float32)
        out[rows, :] = total.astype(jnp.bfloat16)
        return carry

    lax.fori_loop(0, blocks, finish, 0)

    def drain_hot(j, carry):
        give(me, partner, hot_send.at[j]).wait_send()
        return carry

    lax.fori_loop(0, half, drain_hot, 0)

    def drain_pass(j, carry):
        give(me, partner, pass_send.at[j]).wait_send()
        return carry

    lax.fori_loop(1, half, drain_pass, 0)


def solution(mesh):
    n, n_tp = mesh.shape["kv"], mesh.shape["tp"]

    def local(x, wq, wk, wv, wo, scale, hot, chosen):
        tok, depth = x.shape
        own = tok // KB
        width = wk.shape[1] + wv.shape[1]
        blocks, nsel = chosen.shape
        q_cols = wq.shape[1]
        q_chunk = 256
        part_cols = wo.shape[1] // n_tp
        bf16 = jnp.bfloat16
        dma = pltpu.SemaphoreType.DMA
        any_space = pl.BlockSpec(memory_space=pl.ANY)
        vmem = pl.BlockSpec(memory_space=pltpu.VMEM)
        return pl.pallas_call(
            functools.partial(kernel, n, n_tp),
            out_shape=pltpu.VMEM((tok, part_cols), bf16),
            in_specs=[any_space] * 8,
            out_specs=vmem,
            scratch_shapes=[
                pltpu.VMEM((tok, depth), bf16),
                pltpu.VMEM((q_cols // q_chunk, depth, q_chunk), bf16),
                pltpu.VMEM(wk.shape, bf16),
                pltpu.VMEM(wv.shape, bf16),
                pltpu.VMEM((n_tp, wo.shape[0], part_cols), bf16),
                pltpu.VMEM((tok, q_cols), bf16),
                pltpu.VMEM((own, KB, width), bf16),
                pltpu.VMEM((own + HOT_MOST * n, KB, width), bf16),
                pltpu.VMEM((nsel * KB, width), bf16),
                pltpu.VMEM((tok, q_cols), bf16),
                pltpu.VMEM((n_tp - 1, blocks, QB, part_cols), bf16),
                pltpu.VMEM((n_tp - 1, blocks, QB, part_cols), bf16),
                pltpu.VMEM((tok, part_cols), bf16),
                pltpu.VMEM((blocks, QB, nsel * KB), jnp.float32),
                pltpu.SMEM(scale.shape, jnp.float32),
                pltpu.SMEM(hot.shape, jnp.int32),
                pltpu.SMEM(chosen.shape, jnp.int32),
                pltpu.SMEM(hot.shape, jnp.int32),
                dma((3,)),
                dma((3 * PIECES,)),
                dma((q_cols // q_chunk,)),
                dma((n_tp,)),
                dma((n // 2,)),
                dma((n // 2,)),
                dma((n,)),
                dma(((n_tp - 1) * blocks,)),
                dma(((n_tp - 1) * blocks,)),
            ],
            compiler_params=pltpu.CompilerParams(
                collective_id=0, has_side_effects=True, vmem_limit_bytes=32 * 1024 * 1024
            ),
        )(*[pltpu.with_memory_space_constraint(a, pltpu.HBM) for a in (x, wq, wk, wv, wo, scale, hot, chosen)])
    return jax.shard_map(
        local,
        mesh=mesh,
        in_specs=(
            P("kv", None),
            P(None, "tp"),
            P(None, "tp"),
            P(None, "tp"),
            P("tp", None),
            P("tp"),
            P(),
            P("kv", None),
        ),
        out_specs=P("kv", "tp"),
        check_vma=False,
    )
```

```python
import functools

import jax
import jax.numpy as jnp
from jax import lax
from jax.experimental import pallas as pl
from jax.experimental.pallas import tpu as pltpu
from jax.sharding import PartitionSpec as P

HD = 64
KB = 32
QB = 64
HOT_MOST = 2
SEND_LEAD = 2
LANES = 128
PIECES = 4
LOG2E = 1.4426950408889634
MESH = pl.DeviceIdType.MESH


def dot(a, b):
    return jnp.dot(a, b, preferred_element_type=jnp.float32)


def row_of_chips(mesh, n):
    where = [tuple(getattr(d, "coords", ())) for d in mesh.devices.reshape(n, -1)[:, 0]]
    if len(where[0]) != 3:
        return 1
    last = [k for k in range(n) if where[k][2] == where[0][2]]
    wide = len(last) // 2
    even = last == list(range(len(last))) and wide > 0 and n % (2 * wide) == 0
    return wide if even else 1


def kernel(
    n,
    n_tp,
    wide,
    x_hbm,
    wq_hbm,
    wk_hbm,
    wv_hbm,
    wo_hbm,
    scale_hbm,
    hot_hbm,
    chosen_hbm,
    out,
    x,
    wq,
    wk,
    wv,
    wo,
    q,
    local,
    pool,
    kvg,
    heads,
    sent,
    got,
    mine_part,
    bias,
    scale_ref,
    hot_ref,
    chosen_ref,
    slot_ref,
    small_sem,
    load_sem,
    wq_sem,
    wo_sem,
    hot_send,
    pass_send,
    hot_recv,
    part_send,
    part_recv,
    relay_send,
    ready,
):
    me = lax.axis_index("kv")
    t = lax.axis_index("tp")
    own = local.shape[0]
    width = local.shape[2]
    nsel = chosen_ref.shape[1]
    nhot = hot_ref.shape[0]
    blocks = chosen_ref.shape[0]
    head_count = scale_ref.shape[0]
    kv_heads = wk.shape[1] // HD
    pairs = head_count // kv_heads // 2
    keys = nsel * KB
    part_cols = wo.shape[2]
    partner = me + 1 - 2 * lax.rem(me, 2)
    half = n // 2

    depth = x.shape[1] // PIECES
    cuts = [slice(i * depth, (i + 1) * depth) for i in range(PIECES)]
    loads = [
        [
            pltpu.make_async_copy(x_hbm.at[:, cut], x.at[:, cut], load_sem.at[3 * i]),
            pltpu.make_async_copy(wk_hbm.at[cut], wk.at[cut], load_sem.at[3 * i + 1]),
            pltpu.make_async_copy(wv_hbm.at[cut], wv.at[cut], load_sem.at[3 * i + 2]),
        ]
        for i, cut in enumerate(cuts)
    ]
    smalls = [
        pltpu.make_async_copy(hot_hbm, hot_ref, small_sem.at[0]),
        pltpu.make_async_copy(chosen_hbm, chosen_ref, small_sem.at[1]),
        pltpu.make_async_copy(scale_hbm, scale_ref, small_sem.at[2]),
    ]
    for load in loads[0]:
        load.start()
    for small in smalls:
        small.start()
    for piece in loads[1:]:
        for load in piece:
            load.start()
    q_chunk = wq.shape[2]
    wq_loads = [
        pltpu.make_async_copy(wq_hbm.at[:, pl.ds(i * q_chunk, q_chunk)], wq.at[i], wq_sem.at[i])
        for i in range(wq.shape[0])
    ]
    targets = [lax.rem(t + k, n_tp) for k in range(n_tp)]
    order = list(range(1, n_tp)) + [0]
    wo_loads = [
        pltpu.make_async_copy(
            wo_hbm.at[:, pl.ds(pl.multiple_of(targets[k] * part_cols, LANES), part_cols)],
            wo.at[k],
            wo_sem.at[k],
        )
        for k in range(n_tp)
    ]

    barrier = pltpu.get_barrier_semaphore()

    rank = lax.div(me, 2)
    core = lax.rem(me, 2)
    level = lax.div(rank, wide)
    place = lax.rem(rank, wide)
    top = half // wide - 1
    below = jnp.where(level == top, rank, level + place)

    def across(chip):
        return (2 * chip + 1 - core, t)

    def direct(low, high):
        high_level = lax.div(high, wide)
        return (
            (high_level == top)
            | (high_level == lax.div(low, wide))
            | (lax.rem(high, wide) == lax.rem(low, wide))
        )

    def greet(j, carry):
        @pl.when(direct(rank, rank + j))
        def _():
            pl.semaphore_signal(
                barrier, inc=1, device_id=across(rank + j), device_id_type=MESH
            )

        return carry

    lax.fori_loop(1, half - rank, greet, 0)
    pl.semaphore_signal(barrier, inc=1, device_id=(partner, t), device_id_type=MESH)
    for k in range(1, n_tp):
        pl.semaphore_signal(barrier, inc=1, device_id=(me, targets[k]), device_id_type=MESH)


    def tell(j, carry):
        @pl.when(direct(rank - j, rank))
        def _():
            pl.semaphore_signal(
                ready.at[j], inc=1, device_id=across(rank - j), device_id_type=MESH
            )

        return carry

    def meet():
        pl.semaphore_wait(barrier, below + n_tp)
        lax.fori_loop(1, rank + 1, tell, 0)

    pl.when(level > 0)(meet)
    for small in smalls:
        small.wait()
    hots = [hot_ref[h] for h in range(nhot)]
    owners = [lax.div(hot, own) for hot in hots]
    mine = [jnp.int32(0), jnp.int32(0)]
    for h in range(nhot):
        turn = jnp.int32(0)
        for g in range(h):
            turn = turn + (owners[g] == owners[h]).astype(jnp.int32)
        slot_ref[h] = jnp.where(lax.div(owners[h], 2) > rank, 0, own + owners[h] * HOT_MOST + turn)
        offset = hots[h] - owners[h] * own
        for r in range(HOT_MOST):
            mine[r] = jnp.where((owners[h] == me) & (turn == r), offset, mine[r])

    total = None
    for piece, cut in zip(loads, cuts):
        for load in piece:
            load.wait()
        if total is None:
            for load in wq_loads:
                load.start()
            for k in order:
                wo_loads[k].start()
        term = dot(x[:, cut], jnp.concatenate([wk[cut], wv[cut]], axis=1))
        total = term if total is None else total + term
    packed = total.astype(jnp.bfloat16).reshape(own, KB, width)
    local[...] = packed
    pool[pl.ds(0, own)] = packed
    first = own + me * HOT_MOST
    for r in range(HOT_MOST):
        pool[first + r] = local[mine[r]]

    def give(source, device, send):
        rows = pl.ds(own + source * HOT_MOST, HOT_MOST)
        return pltpu.make_async_remote_copy(
            src_ref=pool.at[rows],
            dst_ref=pool.at[rows],
            send_sem=send,
            recv_sem=hot_recv.at[source],
            device_id=(device, t),
            device_id_type=MESH,
        )

    pl.when(level == 0)(meet)
    give(me, partner, hot_send.at[0]).start()
    pieces = wq.shape[0]

    def send_own(j, carry):
        @pl.when(direct(rank, rank + j))
        def _():
            pl.semaphore_wait(ready.at[j], 1)
            give(me, across(rank + j)[0], hot_send.at[j]).start()

        return carry

    def send_some(stage, begin):
        part = (half - 1) * (stage + SEND_LEAD) // (SEND_LEAD + 2)
        upto = jnp.maximum(jnp.minimum(part, half - 1 - rank) + 1, begin)
        lax.fori_loop(begin, upto, send_own, 0)
        return upto

    sent_to = send_some(0, jnp.int32(1))

    lane = lax.broadcasted_iota(jnp.int32, (1, keys), 1)
    in_block = lax.rem(lane, KB)
    entry_of = lax.div(lane, KB)

    def mask(b, carry):
        key_pos = in_block
        for e in range(nsel):
            code = chosen_ref[b, e]
            listed = jnp.clip(code - own, 0, nhot - 1)
            block_id = jnp.where(code < own, me * own + code, hot_ref[listed])
            key_pos = jnp.where(entry_of == e, block_id * KB + in_block, key_pos)
        query_pos = (me * blocks + b) * QB + lax.broadcasted_iota(jnp.int32, (QB, keys), 0)
        bias[b] = jnp.where(key_pos <= query_pos, 0.0, -jnp.inf).astype(jnp.float32)
        return carry

    lax.fori_loop(0, blocks, mask, 0)

    def relay(j, m):
        mate = level * wide + lax.rem(place + m, wide)
        return give(across(rank - j * wide)[0], 2 * mate + core, relay_send.at[j * wide + m])

    def pass_on(j):
        copy = give(across(rank - j)[0], partner, pass_send.at[j])
        copy.wait_recv()
        copy.start()

    def pass_column(j, carry):
        pass_on(j * wide)
        for m in range(1, wide):
            relay(j, m).start()
        return carry

    def pass_rest(j, carry):
        pl.when((level == top) | (lax.rem(j, wide) != 0))(lambda: pass_on(j))
        return carry

    columns = jnp.where(level == top, 0, level)
    done = jnp.int32(1)
    for i in range(pieces):
        wq_loads[i].wait()
        q[:, i * q_chunk : (i + 1) * q_chunk] = dot(x[...], wq[i]).astype(jnp.bfloat16)
        if i < 2:
            sent_to = send_some(i + 1, sent_to)
        if i == 1:
            lax.fori_loop(1, columns + 1, pass_column, 0)
        if i >= 2:
            upto = lax.div(rank * (i - 1), pieces - 2) + 1
            lax.fori_loop(done, upto, pass_rest, 0)
            done = upto

    def land(j, carry):
        give(2 * (rank - j) + core, partner, pass_send.at[0]).wait_recv()
        return carry

    give(partner, partner, pass_send.at[0]).wait_recv()
    lax.fori_loop(1, rank + 1, land, 0)
    for k in range(1, n_tp):
        wo_loads[k].wait()

    low = lax.broadcasted_iota(jnp.int32, (keys, LANES), 1) < HD
    zero = jnp.zeros((keys, LANES), jnp.bfloat16)
    ones = jnp.ones((keys, LANES), jnp.bfloat16)
    ones_low, ones_high = jnp.where(low, ones, zero), jnp.where(low, zero, ones)

    def part_copy(k, b):
        at = (k - 1) * blocks + b
        return pltpu.make_async_remote_copy(
            src_ref=sent.at[k - 1, b],
            dst_ref=got.at[k - 1, b],
            send_sem=part_send.at[at],
            recv_sem=part_recv.at[at],
            device_id=(me, targets[k]),
            device_id_type=MESH,
        )

    def attend(b, carry):
        for e in range(nsel):
            code = chosen_ref[b, e]
            listed = jnp.clip(code - own, 0, nhot - 1)
            row = jnp.where(code < own, code, slot_ref[listed])
            kvg[e * KB : (e + 1) * KB, :] = pool[row]
        rows = pl.ds(pl.multiple_of(b * QB, QB), QB)

        def spread(u):
            tile = kvg[:, (u // 2) * LANES : (u // 2 + 1) * LANES]
            turned = jnp.concatenate([tile[:, HD:], tile[:, :HD]], axis=1)
            if u % 2 == 1:
                tile, turned = turned, tile
            return jnp.where(low, tile, zero), jnp.where(low, zero, turned)

        for c in range(kv_heads):
            k_low, k_high = spread(c)
            k_both = jnp.concatenate([k_low, k_high], axis=0)
            v_low, v_high = spread(kv_heads + c)
            v_both = jnp.concatenate(
                [
                    jnp.concatenate([v_low, ones_low], axis=1),
                    jnp.concatenate([v_high, ones_high], axis=1),
                ],
                axis=0,
            )
            first_pair = c * pairs
            q_rows = jnp.concatenate(
                [
                    q[rows, (first_pair + p) * LANES : (first_pair + p + 1) * LANES]
                    for p in range(pairs)
                ],
                axis=0,
            )
            scores = lax.dot_general(
                q_rows, k_both, (((1,), (1,)), ((), ())), preferred_element_type=jnp.float32
            )
            lifted = []
            for p in range(pairs):
                both = []
                for s in range(2):
                    factor = scale_ref[(first_pair + p) * 2 + s] * (HD**-0.5 * LOG2E)
                    part = scores[p * QB : (p + 1) * QB, s * keys : (s + 1) * keys]
                    part = part * factor + bias[b]
                    top = jnp.max(part, axis=1, keepdims=True)
                    both.append(jnp.exp2(part - top).astype(jnp.bfloat16))
                lifted.append(jnp.concatenate(both, axis=1))
            summed = dot(jnp.concatenate(lifted, axis=0), v_both)
            held = (summed[:, :LANES] / summed[:, LANES:]).astype(jnp.bfloat16)
            for p in range(pairs):
                heads[rows, (first_pair + p) * LANES : (first_pair + p + 1) * LANES] = held[
                    p * QB : (p + 1) * QB
                ]
        for k in range(1, n_tp):
            sent[k - 1, b] = dot(heads[rows, :], wo[k]).astype(jnp.bfloat16)
            part_copy(k, b).start()
        return carry

    lax.fori_loop(0, blocks, attend, 0)

    wo_loads[0].wait()
    mine_part[...] = dot(heads[...], wo[0]).astype(jnp.bfloat16)

    def finish(b, carry):
        rows = pl.ds(pl.multiple_of(b * QB, QB), QB)
        total = mine_part[rows, :].astype(jnp.float32)
        for k in range(1, n_tp):
            part_copy(k, b).wait()
            total = total + got[k - 1, b].astype(jnp.float32)
        out[rows, :] = total.astype(jnp.bfloat16)
        return carry

    lax.fori_loop(0, blocks, finish, 0)

    give(me, partner, hot_send.at[0]).wait_send()

    def drain_hot(j, carry):
        @pl.when(direct(rank, rank + j))
        def _():
            give(me, partner, hot_send.at[j]).wait_send()

        return carry

    lax.fori_loop(1, half - rank, drain_hot, 0)

    def drain_pass(j, carry):
        give(me, partner, pass_send.at[j]).wait_send()
        return carry

    lax.fori_loop(1, rank + 1, drain_pass, 0)

    def drain_relay(j, carry):
        for m in range(1, wide):
            relay(j, m).wait_send()
        return carry

    lax.fori_loop(1, columns + 1, drain_relay, 0)


def solution(mesh):
    n, n_tp = mesh.shape["kv"], mesh.shape["tp"]
    wide = row_of_chips(mesh, n)

    def local(x, wq, wk, wv, wo, scale, hot, chosen):
        tok, depth = x.shape
        own = tok // KB
        width = wk.shape[1] + wv.shape[1]
        blocks, nsel = chosen.shape
        q_cols = wq.shape[1]
        q_chunk = 256
        part_cols = wo.shape[1] // n_tp
        bf16 = jnp.bfloat16
        dma = pltpu.SemaphoreType.DMA
        any_space = pl.BlockSpec(memory_space=pl.ANY)
        vmem = pl.BlockSpec(memory_space=pltpu.VMEM)
        return pl.pallas_call(
            functools.partial(kernel, n, n_tp, wide),
            out_shape=pltpu.VMEM((tok, part_cols), bf16),
            in_specs=[any_space] * 8,
            out_specs=vmem,
            scratch_shapes=[
                pltpu.VMEM((tok, depth), bf16),
                pltpu.VMEM((q_cols // q_chunk, depth, q_chunk), bf16),
                pltpu.VMEM(wk.shape, bf16),
                pltpu.VMEM(wv.shape, bf16),
                pltpu.VMEM((n_tp, wo.shape[0], part_cols), bf16),
                pltpu.VMEM((tok, q_cols), bf16),
                pltpu.VMEM((own, KB, width), bf16),
                pltpu.VMEM((own + HOT_MOST * n, KB, width), bf16),
                pltpu.VMEM((nsel * KB, width), bf16),
                pltpu.VMEM((tok, q_cols), bf16),
                pltpu.VMEM((n_tp - 1, blocks, QB, part_cols), bf16),
                pltpu.VMEM((n_tp - 1, blocks, QB, part_cols), bf16),
                pltpu.VMEM((tok, part_cols), bf16),
                pltpu.VMEM((blocks, QB, nsel * KB), jnp.float32),
                pltpu.SMEM(scale.shape, jnp.float32),
                pltpu.SMEM(hot.shape, jnp.int32),
                pltpu.SMEM(chosen.shape, jnp.int32),
                pltpu.SMEM(hot.shape, jnp.int32),
                dma((3,)),
                dma((3 * PIECES,)),
                dma((q_cols // q_chunk,)),
                dma((n_tp,)),
                dma((n // 2,)),
                dma((n // 2,)),
                dma((n,)),
                dma(((n_tp - 1) * blocks,)),
                dma(((n_tp - 1) * blocks,)),
                dma((n // 2,)),
                pltpu.SemaphoreType.REGULAR((n // 2,)),
            ],
            compiler_params=pltpu.CompilerParams(
                collective_id=0, has_side_effects=True, vmem_limit_bytes=32 * 1024 * 1024
            ),
        )(
            *[
                pltpu.with_memory_space_constraint(a, pltpu.HBM)
                for a in (x, wq, wk, wv, wo, scale, hot, chosen)
            ]
        )

    return jax.shard_map(
        local,
        mesh=mesh,
        in_specs=(
            P("kv", None),
            P(None, "tp"),
            P(None, "tp"),
            P(None, "tp"),
            P("tp", None),
            P("tp"),
            P(),
            P("kv", None),
        ),
        out_specs=P("kv", "tp"),
        check_vma=False,
    )
```

```python
import functools

import jax
import jax.numpy as jnp
from jax import lax
from jax.experimental import pallas as pl
from jax.experimental.pallas import tpu as pltpu
from jax.sharding import PartitionSpec as P

HD = 64
KB = 32
QB = 64
QR = 32
HOT_MOST = 2
LANES = 128
PIECES = 4
LOG2E = 1.4426950408889634
MESH = pl.DeviceIdType.MESH


def dot(a, b):
    return jnp.dot(a, b, preferred_element_type=jnp.float32)


def row_of_chips(mesh, n):
    where = [tuple(getattr(d, "coords", ())) for d in mesh.devices.reshape(n, -1)[:, 0]]
    if len(where[0]) != 3:
        return 1
    last = [k for k in range(n) if where[k][2] == where[0][2]]
    wide = len(last) // 2
    even = last == list(range(len(last))) and wide > 0 and n % (2 * wide) == 0
    return wide if even else 1


def kernel(
    n,
    n_tp,
    wide,
    x_hbm,
    wq_hbm,
    wk_hbm,
    wv_hbm,
    wo_hbm,
    scale_hbm,
    hot_hbm,
    chosen_hbm,
    out,
    x,
    wq,
    wk,
    wv,
    wo,
    q,
    local,
    pool,
    kvg,
    heads,
    sent,
    got,
    mine_part,
    bias,
    scale_ref,
    hot_ref,
    chosen_ref,
    slot_ref,
    small_sem,
    load_sem,
    wq_sem,
    wo_sem,
    hot_send,
    pass_send,
    hot_recv,
    part_send,
    part_recv,
    relay_send,
    ready,
    ready_tp,
):
    me = lax.axis_index("kv")
    t = lax.axis_index("tp")
    own = local.shape[0]
    width = local.shape[2]
    nsel = chosen_ref.shape[1]
    nhot = hot_ref.shape[0]
    blocks = chosen_ref.shape[0]
    head_count = scale_ref.shape[0]
    kv_heads = wk.shape[1] // HD
    pairs = head_count // kv_heads // 2
    keys = nsel * KB
    part_cols = wo.shape[2]
    partner = me + 1 - 2 * lax.rem(me, 2)
    half = n // 2

    depth = x.shape[1] // PIECES
    cuts = [slice(i * depth, (i + 1) * depth) for i in range(PIECES)]
    loads = [
        [
            pltpu.make_async_copy(x_hbm.at[:, cut], x.at[:, cut], load_sem.at[3 * i]),
            pltpu.make_async_copy(wk_hbm.at[cut], wk.at[cut], load_sem.at[3 * i + 1]),
            pltpu.make_async_copy(wv_hbm.at[cut], wv.at[cut], load_sem.at[3 * i + 2]),
        ]
        for i, cut in enumerate(cuts)
    ]
    smalls = [
        pltpu.make_async_copy(hot_hbm, hot_ref, small_sem.at[0]),
        pltpu.make_async_copy(chosen_hbm, chosen_ref, small_sem.at[1]),
        pltpu.make_async_copy(scale_hbm, scale_ref, small_sem.at[2]),
    ]
    for load in loads[0]:
        load.start()
    for small in smalls:
        small.start()
    for piece in loads[1:]:
        for load in piece:
            load.start()
    q_chunk = wq.shape[2]
    wq_loads = [
        pltpu.make_async_copy(wq_hbm.at[:, pl.ds(i * q_chunk, q_chunk)], wq.at[i], wq_sem.at[i])
        for i in range(wq.shape[0])
    ]
    targets = [lax.rem(t + k, n_tp) for k in range(n_tp)]
    order = list(range(1, n_tp)) + [0]
    wo_loads = [
        pltpu.make_async_copy(
            wo_hbm.at[:, pl.ds(pl.multiple_of(targets[k] * part_cols, LANES), part_cols)],
            wo.at[k],
            wo_sem.at[k],
        )
        for k in range(n_tp)
    ]

    barrier = pltpu.get_barrier_semaphore()

    rank = lax.div(me, 2)
    core = lax.rem(me, 2)
    level = lax.div(rank, wide)
    place = lax.rem(rank, wide)
    top = half // wide - 1
    below = jnp.where(level == top, rank, level + place)

    def across(chip):
        return (2 * chip + 1 - core, t)

    def direct(low, high):
        high_level = lax.div(high, wide)
        return (
            (high_level == top)
            | (high_level == lax.div(low, wide))
            | (lax.rem(high, wide) == lax.rem(low, wide))
        )

    def greet(j, carry):
        @pl.when(direct(rank, rank + j))
        def _():
            pl.semaphore_signal(
                barrier, inc=1, device_id=across(rank + j), device_id_type=MESH
            )

        return carry

    lax.fori_loop(1, half - rank, greet, 0)
    pl.semaphore_signal(barrier, inc=1, device_id=(partner, t), device_id_type=MESH)
    for k in range(1, n_tp):

        @pl.when(targets[k] > t)
        def _(other=targets[k]):
            pl.semaphore_signal(barrier, inc=1, device_id=(me, other), device_id_type=MESH)


    def tell(j, carry):
        @pl.when(direct(rank - j, rank))
        def _():
            pl.semaphore_signal(
                ready.at[j], inc=1, device_id=across(rank - j), device_id_type=MESH
            )

        return carry

    def meet():
        pl.semaphore_wait(barrier, below + 1 + t)
        lax.fori_loop(1, rank + 1, tell, 0)
        for k in range(1, n_tp):

            @pl.when(targets[k] < t)
            def _(other=targets[k]):
                pl.semaphore_signal(
                    ready_tp.at[t], inc=1, device_id=(me, other), device_id_type=MESH
                )


    pl.when(rank > 0)(meet)
    for small in smalls:
        small.wait()
    hots = [hot_ref[h] for h in range(nhot)]
    owners = [lax.div(hot, own) for hot in hots]
    mine = [jnp.int32(0), jnp.int32(0)]
    for h in range(nhot):
        turn = jnp.int32(0)
        for g in range(h):
            turn = turn + (owners[g] == owners[h]).astype(jnp.int32)
        slot_ref[h] = jnp.where(lax.div(owners[h], 2) > rank, 0, own + owners[h] * HOT_MOST + turn)
        offset = hots[h] - owners[h] * own
        for r in range(HOT_MOST):
            mine[r] = jnp.where((owners[h] == me) & (turn == r), offset, mine[r])

    total = None
    for piece, cut in zip(loads, cuts):
        for load in piece:
            load.wait()
        if total is None:
            for load in wq_loads:
                load.start()
            for k in order:
                wo_loads[k].start()
        term = dot(x[:, cut], jnp.concatenate([wk[cut], wv[cut]], axis=1))
        total = term if total is None else total + term
    packed = total.astype(jnp.bfloat16).reshape(own, KB, width)
    local[...] = packed
    pool[pl.ds(0, own)] = packed
    first = own + me * HOT_MOST
    for r in range(HOT_MOST):
        pool[first + r] = local[mine[r]]

    def give(source, device, send):
        rows = pl.ds(own + source * HOT_MOST, HOT_MOST)
        return pltpu.make_async_remote_copy(
            src_ref=pool.at[rows],
            dst_ref=pool.at[rows],
            send_sem=send,
            recv_sem=hot_recv.at[source],
            device_id=(device, t),
            device_id_type=MESH,
        )

    pl.when(rank == 0)(meet)
    give(me, partner, hot_send.at[0]).start()

    def send_own(j, carry):
        @pl.when(direct(rank, rank + j))
        def _():
            pl.semaphore_wait(ready.at[j], 1)
            give(me, across(rank + j)[0], hot_send.at[j]).start()

        return carry

    first = jnp.where(level == 0, 1, half - rank)
    lax.fori_loop(1, first, send_own, 0)

    lane = lax.broadcasted_iota(jnp.int32, (1, keys), 1)
    in_block = lax.rem(lane, KB)
    entry_of = lax.div(lane, KB)

    def mask(b, carry):
        key_pos = in_block
        for e in range(nsel):
            code = chosen_ref[b, e]
            listed = jnp.clip(code - own, 0, nhot - 1)
            block_id = jnp.where(code < own, me * own + code, hot_ref[listed])
            key_pos = jnp.where(entry_of == e, block_id * KB + in_block, key_pos)
        query_pos = (me * blocks + b) * QB + lax.broadcasted_iota(jnp.int32, (QB, keys), 0)
        bias[b] = jnp.where(key_pos <= query_pos, 0.0, -jnp.inf).astype(jnp.float32)
        return carry

    lax.fori_loop(0, blocks, mask, 0)

    def relay(j, m):
        mate = level * wide + lax.rem(place + m, wide)
        return give(across(rank - j * wide)[0], 2 * mate + core, relay_send.at[j * wide + m])

    def pass_on(j):
        copy = give(across(rank - j)[0], partner, pass_send.at[j])
        copy.wait_recv()
        copy.start()

    def pass_column(j, carry):
        pass_on(j * wide)
        for m in range(1, wide):
            relay(j, m).start()
        return carry

    def pass_rest(j, carry):
        pl.when((level == top) | (lax.rem(j, wide) != 0))(lambda: pass_on(j))
        return carry

    columns = jnp.where(level == top, 0, level)
    for i in range(wq.shape[0]):
        wq_loads[i].wait()
        q[:, i * q_chunk : (i + 1) * q_chunk] = dot(x[...], wq[i]).astype(jnp.bfloat16)
        if i == 0:
            lax.fori_loop(first, half - rank, send_own, 0)
            lax.fori_loop(1, columns + 1, pass_column, 0)
    lax.fori_loop(1, rank + 1, pass_rest, 0)

    def land(j, carry):
        give(2 * (rank - j) + core, partner, pass_send.at[0]).wait_recv()
        return carry

    give(partner, partner, pass_send.at[0]).wait_recv()
    lax.fori_loop(1, rank + 1, land, 0)
    for k in range(1, n_tp):
        wo_loads[k].wait()

    low = lax.broadcasted_iota(jnp.int32, (keys, LANES), 1) < HD
    zero = jnp.zeros((keys, LANES), jnp.bfloat16)
    ones = jnp.ones((keys, LANES), jnp.bfloat16)
    ones_low, ones_high = jnp.where(low, ones, zero), jnp.where(low, zero, ones)

    steps = sent.shape[1]
    for k in range(1, n_tp):

        @pl.when(targets[k] > t)
        def _(other=targets[k]):
            pl.semaphore_wait(ready_tp.at[other], 1)


    def part_copy(k, b):
        at = (k - 1) * steps + b
        return pltpu.make_async_remote_copy(
            src_ref=sent.at[k - 1, b],
            dst_ref=got.at[k - 1, b],
            send_sem=part_send.at[at],
            recv_sem=part_recv.at[at],
            device_id=(me, targets[k]),
            device_id_type=MESH,
        )

    def attend(step, carry):
        b = lax.div(step, QB // QR)
        half_rows = pl.ds(pl.multiple_of(lax.rem(step, QB // QR) * QR, QR), QR)
        lift = bias[b, half_rows, :]
        for e in range(nsel):
            code = chosen_ref[b, e]
            listed = jnp.clip(code - own, 0, nhot - 1)
            row = jnp.where(code < own, code, slot_ref[listed])
            kvg[e * KB : (e + 1) * KB, :] = pool[row]
        rows = pl.ds(pl.multiple_of(step * QR, QR), QR)

        def spread(u):
            tile = kvg[:, (u // 2) * LANES : (u // 2 + 1) * LANES]
            turned = jnp.concatenate([tile[:, HD:], tile[:, :HD]], axis=1)
            if u % 2 == 1:
                tile, turned = turned, tile
            return jnp.where(low, tile, zero), jnp.where(low, zero, turned)

        for c in range(kv_heads):
            k_low, k_high = spread(c)
            k_both = jnp.concatenate([k_low, k_high], axis=0)
            v_low, v_high = spread(kv_heads + c)
            v_both = jnp.concatenate(
                [
                    jnp.concatenate([v_low, ones_low], axis=1),
                    jnp.concatenate([v_high, ones_high], axis=1),
                ],
                axis=0,
            )
            first_pair = c * pairs
            q_rows = jnp.concatenate(
                [
                    q[rows, (first_pair + p) * LANES : (first_pair + p + 1) * LANES]
                    for p in range(pairs)
                ],
                axis=0,
            )
            scores = lax.dot_general(
                q_rows, k_both, (((1,), (1,)), ((), ())), preferred_element_type=jnp.float32
            )
            lifted = []
            for p in range(pairs):
                both = []
                for s in range(2):
                    factor = scale_ref[(first_pair + p) * 2 + s] * (HD**-0.5 * LOG2E)
                    part = scores[p * QR : (p + 1) * QR, s * keys : (s + 1) * keys]
                    part = part * factor + lift
                    top = jnp.max(part, axis=1, keepdims=True)
                    both.append(jnp.exp2(part - top).astype(jnp.bfloat16))
                lifted.append(jnp.concatenate(both, axis=1))
            summed = dot(jnp.concatenate(lifted, axis=0), v_both)
            held = (summed[:, :LANES] / summed[:, LANES:]).astype(jnp.bfloat16)
            for p in range(pairs):
                heads[rows, (first_pair + p) * LANES : (first_pair + p + 1) * LANES] = held[
                    p * QR : (p + 1) * QR
                ]
        for k in range(1, n_tp):
            sent[k - 1, step] = dot(heads[rows, :], wo[k]).astype(jnp.bfloat16)
            part_copy(k, step).start()
        return carry

    lax.fori_loop(0, steps, attend, 0)

    wo_loads[0].wait()
    mine_part[...] = dot(heads[...], wo[0]).astype(jnp.bfloat16)

    def finish(b, carry):
        rows = pl.ds(pl.multiple_of(b * QR, QR), QR)
        total = mine_part[rows, :].astype(jnp.float32)
        for k in range(1, n_tp):
            part_copy(k, b).wait()
            total = total + got[k - 1, b].astype(jnp.float32)
        out[rows, :] = total.astype(jnp.bfloat16)
        return carry

    lax.fori_loop(0, steps, finish, 0)

    give(me, partner, hot_send.at[0]).wait_send()

    def drain_hot(j, carry):
        @pl.when(direct(rank, rank + j))
        def _():
            give(me, partner, hot_send.at[j]).wait_send()

        return carry

    lax.fori_loop(1, half - rank, drain_hot, 0)

    def drain_pass(j, carry):
        give(me, partner, pass_send.at[j]).wait_send()
        return carry

    lax.fori_loop(1, rank + 1, drain_pass, 0)

    def drain_relay(j, carry):
        for m in range(1, wide):
            relay(j, m).wait_send()
        return carry

    lax.fori_loop(1, columns + 1, drain_relay, 0)


def solution(mesh):
    n, n_tp = mesh.shape["kv"], mesh.shape["tp"]
    wide = row_of_chips(mesh, n)

    def local(x, wq, wk, wv, wo, scale, hot, chosen):
        tok, depth = x.shape
        own = tok // KB
        width = wk.shape[1] + wv.shape[1]
        blocks, nsel = chosen.shape
        q_cols = wq.shape[1]
        q_chunk = 512
        part_cols = wo.shape[1] // n_tp
        bf16 = jnp.bfloat16
        dma = pltpu.SemaphoreType.DMA
        any_space = pl.BlockSpec(memory_space=pl.ANY)
        vmem = pl.BlockSpec(memory_space=pltpu.VMEM)
        return pl.pallas_call(
            functools.partial(kernel, n, n_tp, wide),
            out_shape=pltpu.VMEM((tok, part_cols), bf16),
            in_specs=[any_space] * 8,
            out_specs=vmem,
            scratch_shapes=[
                pltpu.VMEM((tok, depth), bf16),
                pltpu.VMEM((q_cols // q_chunk, depth, q_chunk), bf16),
                pltpu.VMEM(wk.shape, bf16),
                pltpu.VMEM(wv.shape, bf16),
                pltpu.VMEM((n_tp, wo.shape[0], part_cols), bf16),
                pltpu.VMEM((tok, q_cols), bf16),
                pltpu.VMEM((own, KB, width), bf16),
                pltpu.VMEM((own + HOT_MOST * n, KB, width), bf16),
                pltpu.VMEM((nsel * KB, width), bf16),
                pltpu.VMEM((tok, q_cols), bf16),
                pltpu.VMEM((n_tp - 1, tok // QR, QR, part_cols), bf16),
                pltpu.VMEM((n_tp - 1, tok // QR, QR, part_cols), bf16),
                pltpu.VMEM((tok, part_cols), bf16),
                pltpu.VMEM((blocks, QB, nsel * KB), jnp.float32),
                pltpu.SMEM(scale.shape, jnp.float32),
                pltpu.SMEM(hot.shape, jnp.int32),
                pltpu.SMEM(chosen.shape, jnp.int32),
                pltpu.SMEM(hot.shape, jnp.int32),
                dma((3,)),
                dma((3 * PIECES,)),
                dma((q_cols // q_chunk,)),
                dma((n_tp,)),
                dma((n // 2,)),
                dma((n // 2,)),
                dma((n,)),
                dma(((n_tp - 1) * (tok // QR),)),
                dma(((n_tp - 1) * (tok // QR),)),
                dma((n // 2,)),
                pltpu.SemaphoreType.REGULAR((n // 2,)),
                pltpu.SemaphoreType.REGULAR((n_tp,)),
            ],
            compiler_params=pltpu.CompilerParams(
                collective_id=0, has_side_effects=True, vmem_limit_bytes=32 * 1024 * 1024
            ),
        )(
            *[
                pltpu.with_memory_space_constraint(a, pltpu.HBM)
                for a in (x, wq, wk, wv, wo, scale, hot, chosen)
            ]
        )

    return jax.shard_map(
        local,
        mesh=mesh,
        in_specs=(
            P("kv", None),
            P(None, "tp"),
            P(None, "tp"),
            P(None, "tp"),
            P("tp", None),
            P("tp"),
            P(),
            P("kv", None),
        ),
        out_specs=P("kv", "tp"),
        check_vma=False,
    )
```

```python
import functools

import jax
import jax.numpy as jnp
from jax import lax
from jax.experimental import pallas as pl
from jax.experimental.pallas import tpu as pltpu
from jax.sharding import PartitionSpec as P

HD = 64
KB = 32
QB = 64
QR = 32
HOT_MOST = 2
LANES = 128
PIECES = 4
LOG2E = 1.4426950408889634
MESH = pl.DeviceIdType.MESH


def dot(a, b):
    return jnp.dot(a, b, preferred_element_type=jnp.float32)


def row_of_chips(mesh, n):
    where = [tuple(getattr(d, "coords", ())) for d in mesh.devices.reshape(n, -1)[:, 0]]
    if len(where[0]) != 3:
        return 1
    last = [k for k in range(n) if where[k][2] == where[0][2]]
    wide = len(last) // 2
    even = last == list(range(len(last))) and wide > 0 and n % (2 * wide) == 0
    return wide if even else 1


def kernel(
    n,
    n_tp,
    wide,
    x_hbm,
    wq_hbm,
    wk_hbm,
    wv_hbm,
    wo_hbm,
    scale_hbm,
    hot_hbm,
    chosen_hbm,
    out,
    x,
    wq,
    wk,
    wv,
    wo,
    q,
    local,
    pool,
    kvg,
    heads,
    sent,
    got,
    mine_part,
    bias,
    scale_ref,
    hot_ref,
    chosen_ref,
    slot_ref,
    small_sem,
    load_sem,
    wq_sem,
    wo_sem,
    hot_send,
    pass_send,
    hot_recv,
    part_send,
    part_recv,
    relay_send,
    ready,
    ready_tp,
):
    me = lax.axis_index("kv")
    t = lax.axis_index("tp")
    own = local.shape[0]
    width = local.shape[2]
    nsel = chosen_ref.shape[1]
    nhot = hot_ref.shape[0]
    blocks = chosen_ref.shape[0]
    head_count = scale_ref.shape[0]
    kv_heads = wk.shape[1] // HD
    pairs = head_count // kv_heads // 2
    keys = nsel * KB
    part_cols = wo.shape[2]
    partner = me + 1 - 2 * lax.rem(me, 2)
    half = n // 2

    depth = x.shape[1] // PIECES
    cuts = [slice(i * depth, (i + 1) * depth) for i in range(PIECES)]
    loads = [
        [
            pltpu.make_async_copy(x_hbm.at[:, cut], x.at[:, cut], load_sem.at[3 * i]),
            pltpu.make_async_copy(wk_hbm.at[cut], wk.at[cut], load_sem.at[3 * i + 1]),
            pltpu.make_async_copy(wv_hbm.at[cut], wv.at[cut], load_sem.at[3 * i + 2]),
        ]
        for i, cut in enumerate(cuts)
    ]
    smalls = [
        pltpu.make_async_copy(hot_hbm, hot_ref, small_sem.at[0]),
        pltpu.make_async_copy(chosen_hbm, chosen_ref, small_sem.at[1]),
        pltpu.make_async_copy(scale_hbm, scale_ref, small_sem.at[2]),
    ]
    for load in loads[0]:
        load.start()
    for small in smalls:
        small.start()
    for piece in loads[1:]:
        for load in piece:
            load.start()
    q_chunk = wq.shape[2]
    wq_loads = [
        pltpu.make_async_copy(wq_hbm.at[:, pl.ds(i * q_chunk, q_chunk)], wq.at[i], wq_sem.at[i])
        for i in range(wq.shape[0])
    ]
    targets = [lax.rem(t + k, n_tp) for k in range(n_tp)]
    order = list(range(1, n_tp)) + [0]
    wo_loads = [
        pltpu.make_async_copy(
            wo_hbm.at[:, pl.ds(pl.multiple_of(targets[k] * part_cols, LANES), part_cols)],
            wo.at[k],
            wo_sem.at[k],
        )
        for k in range(n_tp)
    ]

    barrier = pltpu.get_barrier_semaphore()

    rank = lax.div(me, 2)
    core = lax.rem(me, 2)
    level = lax.div(rank, wide)
    place = lax.rem(rank, wide)
    top = half // wide - 1
    below = jnp.where(level == top, rank, level + place)

    def across(chip):
        return (2 * chip + 1 - core, t)

    def direct(low, high):
        high_level = lax.div(high, wide)
        return (
            (high_level == top)
            | (high_level == lax.div(low, wide))
            | (lax.rem(high, wide) == lax.rem(low, wide))
        )

    def greet(j, carry):
        @pl.when(direct(rank, rank + j))
        def _():
            pl.semaphore_signal(
                barrier, inc=1, device_id=across(rank + j), device_id_type=MESH
            )

        return carry

    lax.fori_loop(1, half - rank, greet, 0)
    pl.semaphore_signal(barrier, inc=1, device_id=(partner, t), device_id_type=MESH)
    for k in range(1, n_tp):

        @pl.when(targets[k] > t)
        def _(other=targets[k]):
            pl.semaphore_signal(barrier, inc=1, device_id=(me, other), device_id_type=MESH)


    def tell(j, carry):
        @pl.when(direct(rank - j, rank))
        def _():
            pl.semaphore_signal(
                ready.at[j], inc=1, device_id=across(rank - j), device_id_type=MESH
            )

        return carry

    def meet():
        pl.semaphore_wait(barrier, below + 1 + t)
        lax.fori_loop(1, rank + 1, tell, 0)
        for k in range(1, n_tp):

            @pl.when(targets[k] < t)
            def _(other=targets[k]):
                pl.semaphore_signal(
                    ready_tp.at[t], inc=1, device_id=(me, other), device_id_type=MESH
                )


    pl.when(rank > 0)(meet)
    for small in smalls:
        small.wait()
    hots = [hot_ref[h] for h in range(nhot)]
    owners = [lax.div(hot, own) for hot in hots]
    mine = [jnp.int32(0), jnp.int32(0)]
    for h in range(nhot):
        turn = jnp.int32(0)
        for g in range(h):
            turn = turn + (owners[g] == owners[h]).astype(jnp.int32)
        slot_ref[h] = jnp.where(lax.div(owners[h], 2) > rank, 0, own + owners[h] * HOT_MOST + turn)
        offset = hots[h] - owners[h] * own
        for r in range(HOT_MOST):
            mine[r] = jnp.where((owners[h] == me) & (turn == r), offset, mine[r])

    total = None
    middle = x.shape[0] // 2
    for piece, cut in zip(loads, cuts):
        for load in piece:
            load.wait()
        if piece is loads[0]:
            for load in wq_loads:
                load.start()
            for k in order:
                wo_loads[k].start()
        both = jnp.concatenate([wk[cut], wv[cut]], axis=1)
        term = [dot(x[:middle, cut], both), dot(x[middle:, cut], both)]
        total = term if total is None else [a + b for a, b in zip(total, term)]
    packed = jnp.concatenate(total, axis=0).astype(jnp.bfloat16).reshape(own, KB, width)
    local[...] = packed
    pool[pl.ds(0, own)] = packed
    first = own + me * HOT_MOST
    for r in range(HOT_MOST):
        pool[first + r] = local[mine[r]]

    def give(source, device, send):
        rows = pl.ds(own + source * HOT_MOST, HOT_MOST)
        return pltpu.make_async_remote_copy(
            src_ref=pool.at[rows],
            dst_ref=pool.at[rows],
            send_sem=send,
            recv_sem=hot_recv.at[source],
            device_id=(device, t),
            device_id_type=MESH,
        )

    pl.when(rank == 0)(meet)
    give(me, partner, hot_send.at[0]).start()

    def send_own(j, carry):
        @pl.when(direct(rank, rank + j))
        def _():
            pl.semaphore_wait(ready.at[j], 1)
            give(me, across(rank + j)[0], hot_send.at[j]).start()

        return carry

    first = jnp.where(level == 0, jnp.maximum(top * wide - rank, 1), half - rank)
    lax.fori_loop(1, first, send_own, 0)

    lane = lax.broadcasted_iota(jnp.int32, (1, keys), 1)
    in_block = lax.rem(lane, KB)
    entry_of = lax.div(lane, KB)

    def mask(b, carry):
        key_pos = in_block
        for e in range(nsel):
            code = chosen_ref[b, e]
            listed = jnp.clip(code - own, 0, nhot - 1)
            block_id = jnp.where(code < own, me * own + code, hot_ref[listed])
            key_pos = jnp.where(entry_of == e, block_id * KB + in_block, key_pos)
        query_pos = (me * blocks + b) * QB + lax.broadcasted_iota(jnp.int32, (QB, keys), 0)
        bias[b] = jnp.where(key_pos <= query_pos, 0.0, -jnp.inf).astype(jnp.float32)
        return carry

    lax.fori_loop(0, blocks, mask, 0)

    def relay(j, m):
        mate = level * wide + lax.rem(place + m, wide)
        return give(across(rank - j * wide)[0], 2 * mate + core, relay_send.at[j * wide + m])

    def pass_on(j):
        copy = give(across(rank - j)[0], partner, pass_send.at[j])
        copy.wait_recv()
        copy.start()

    def pass_column(j, carry):
        pass_on(j * wide)
        for m in range(1, wide):
            relay(j, m).start()
        return carry

    def pass_rest(j, carry):
        pl.when((level == top) | (lax.rem(j, wide) != 0))(lambda: pass_on(j))
        return carry

    columns = jnp.where(level == top, 0, level)
    for i in range(wq.shape[0]):
        wq_loads[i].wait()
        q[:, i * q_chunk : (i + 1) * q_chunk] = dot(x[...], wq[i]).astype(jnp.bfloat16)
        if i == 0:
            lax.fori_loop(first, half - rank, send_own, 0)
            lax.fori_loop(1, columns + 1, pass_column, 0)
    lax.fori_loop(1, rank + 1, pass_rest, 0)

    def land(j, carry):
        give(2 * (rank - j) + core, partner, pass_send.at[0]).wait_recv()
        return carry

    give(partner, partner, pass_send.at[0]).wait_recv()
    lax.fori_loop(1, rank + 1, land, 0)
    for k in range(1, n_tp):
        wo_loads[k].wait()

    low = lax.broadcasted_iota(jnp.int32, (keys, LANES), 1) < HD
    zero = jnp.zeros((keys, LANES), jnp.bfloat16)
    ones = jnp.ones((keys, LANES), jnp.bfloat16)
    ones_low, ones_high = jnp.where(low, ones, zero), jnp.where(low, zero, ones)

    steps = sent.shape[1]
    for k in range(1, n_tp):

        @pl.when(targets[k] > t)
        def _(other=targets[k]):
            pl.semaphore_wait(ready_tp.at[other], 1)


    def part_copy(k, b):
        at = (k - 1) * steps + b
        return pltpu.make_async_remote_copy(
            src_ref=sent.at[k - 1, b],
            dst_ref=got.at[k - 1, b],
            send_sem=part_send.at[at],
            recv_sem=part_recv.at[at],
            device_id=(me, targets[k]),
            device_id_type=MESH,
        )

    def attend(step, carry):
        b = lax.div(step, QB // QR)
        half_rows = pl.ds(pl.multiple_of(lax.rem(step, QB // QR) * QR, QR), QR)
        lift = bias[b, half_rows, :]
        for e in range(nsel):
            code = chosen_ref[b, e]
            listed = jnp.clip(code - own, 0, nhot - 1)
            row = jnp.where(code < own, code, slot_ref[listed])
            kvg[e * KB : (e + 1) * KB, :] = pool[row]
        rows = pl.ds(pl.multiple_of(step * QR, QR), QR)

        def spread(u):
            tile = kvg[:, (u // 2) * LANES : (u // 2 + 1) * LANES]
            turned = jnp.concatenate([tile[:, HD:], tile[:, :HD]], axis=1)
            if u % 2 == 1:
                tile, turned = turned, tile
            return jnp.where(low, tile, zero), jnp.where(low, zero, turned)

        for c in range(kv_heads):
            k_low, k_high = spread(c)
            k_both = jnp.concatenate([k_low, k_high], axis=0)
            v_low, v_high = spread(kv_heads + c)
            v_parts = [
                jnp.concatenate([v_low, ones_low], axis=1),
                jnp.concatenate([v_high, ones_high], axis=1),
            ]
            first_pair = c * pairs
            q_rows = jnp.concatenate(
                [
                    q[rows, (first_pair + p) * LANES : (first_pair + p + 1) * LANES]
                    for p in range(pairs)
                ],
                axis=0,
            )
            scores = lax.dot_general(
                q_rows, k_both, (((1,), (1,)), ((), ())), preferred_element_type=jnp.float32
            )
            lifted = []
            for p in range(pairs):
                both = []
                for s in range(2):
                    factor = scale_ref[(first_pair + p) * 2 + s] * (HD**-0.5 * LOG2E)
                    part = scores[p * QR : (p + 1) * QR, s * keys : (s + 1) * keys]
                    part = part * factor + lift
                    top = jnp.max(part, axis=1, keepdims=True)
                    both.append(jnp.exp2(part - top).astype(jnp.bfloat16))
                lifted.append(both)
            summed = sum(
                dot(jnp.concatenate([pair[s] for pair in lifted], axis=0), v_parts[s])
                for s in range(2)
            )
            held = (summed[:, :LANES] / summed[:, LANES:]).astype(jnp.bfloat16)
            for p in range(pairs):
                heads[rows, (first_pair + p) * LANES : (first_pair + p + 1) * LANES] = held[
                    p * QR : (p + 1) * QR
                ]
        for k in range(1, n_tp):
            sent[k - 1, step] = dot(heads[rows, :], wo[k]).astype(jnp.bfloat16)
            part_copy(k, step).start()
        return carry

    lax.fori_loop(0, steps, attend, 0)

    wo_loads[0].wait()
    mine_part[...] = dot(heads[...], wo[0]).astype(jnp.bfloat16)

    def finish(b, carry):
        rows = pl.ds(pl.multiple_of(b * QR, QR), QR)
        total = mine_part[rows, :].astype(jnp.float32)
        for k in range(1, n_tp):
            part_copy(k, b).wait()
            total = total + got[k - 1, b].astype(jnp.float32)
        out[rows, :] = total.astype(jnp.bfloat16)
        return carry

    lax.fori_loop(0, steps, finish, 0)

    give(me, partner, hot_send.at[0]).wait_send()

    def drain_hot(j, carry):
        @pl.when(direct(rank, rank + j))
        def _():
            give(me, partner, hot_send.at[j]).wait_send()

        return carry

    lax.fori_loop(1, half - rank, drain_hot, 0)

    def drain_pass(j, carry):
        give(me, partner, pass_send.at[j]).wait_send()
        return carry

    lax.fori_loop(1, rank + 1, drain_pass, 0)

    def drain_relay(j, carry):
        for m in range(1, wide):
            relay(j, m).wait_send()
        return carry

    lax.fori_loop(1, columns + 1, drain_relay, 0)


def solution(mesh):
    n, n_tp = mesh.shape["kv"], mesh.shape["tp"]
    wide = row_of_chips(mesh, n)

    def local(x, wq, wk, wv, wo, scale, hot, chosen):
        tok, depth = x.shape
        own = tok // KB
        width = wk.shape[1] + wv.shape[1]
        blocks, nsel = chosen.shape
        q_cols = wq.shape[1]
        q_chunk = 512
        part_cols = wo.shape[1] // n_tp
        bf16 = jnp.bfloat16
        dma = pltpu.SemaphoreType.DMA
        any_space = pl.BlockSpec(memory_space=pl.ANY)
        vmem = pl.BlockSpec(memory_space=pltpu.VMEM)
        return pl.pallas_call(
            functools.partial(kernel, n, n_tp, wide),
            out_shape=pltpu.VMEM((tok, part_cols), bf16),
            in_specs=[any_space] * 8,
            out_specs=vmem,
            scratch_shapes=[
                pltpu.VMEM((tok, depth), bf16),
                pltpu.VMEM((q_cols // q_chunk, depth, q_chunk), bf16),
                pltpu.VMEM(wk.shape, bf16),
                pltpu.VMEM(wv.shape, bf16),
                pltpu.VMEM((n_tp, wo.shape[0], part_cols), bf16),
                pltpu.VMEM((tok, q_cols), bf16),
                pltpu.VMEM((own, KB, width), bf16),
                pltpu.VMEM((own + HOT_MOST * n, KB, width), bf16),
                pltpu.VMEM((nsel * KB, width), bf16),
                pltpu.VMEM((tok, q_cols), bf16),
                pltpu.VMEM((n_tp - 1, tok // QR, QR, part_cols), bf16),
                pltpu.VMEM((n_tp - 1, tok // QR, QR, part_cols), bf16),
                pltpu.VMEM((tok, part_cols), bf16),
                pltpu.VMEM((blocks, QB, nsel * KB), jnp.float32),
                pltpu.SMEM(scale.shape, jnp.float32),
                pltpu.SMEM(hot.shape, jnp.int32),
                pltpu.SMEM(chosen.shape, jnp.int32),
                pltpu.SMEM(hot.shape, jnp.int32),
                dma((3,)),
                dma((3 * PIECES,)),
                dma((q_cols // q_chunk,)),
                dma((n_tp,)),
                dma((n // 2,)),
                dma((n // 2,)),
                dma((n,)),
                dma(((n_tp - 1) * (tok // QR),)),
                dma(((n_tp - 1) * (tok // QR),)),
                dma((n // 2,)),
                pltpu.SemaphoreType.REGULAR((n // 2,)),
                pltpu.SemaphoreType.REGULAR((n_tp,)),
            ],
            compiler_params=pltpu.CompilerParams(
                collective_id=0, has_side_effects=True, vmem_limit_bytes=32 * 1024 * 1024
            ),
        )(
            *[
                pltpu.with_memory_space_constraint(a, pltpu.HBM)
                for a in (x, wq, wk, wv, wo, scale, hot, chosen)
            ]
        )

    return jax.shard_map(
        local,
        mesh=mesh,
        in_specs=(
            P("kv", None),
            P(None, "tp"),
            P(None, "tp"),
            P(None, "tp"),
            P("tp", None),
            P("tp"),
            P(),
            P("kv", None),
        ),
        out_specs=P("kv", "tp"),
        check_vma=False,
    )
```

```python
import functools

import jax
import jax.numpy as jnp
from jax import lax
from jax.experimental import pallas as pl
from jax.experimental.pallas import tpu as pltpu
from jax.sharding import PartitionSpec as P

HD = 64
KB = 32
QB = 64
QR = 32
HOT_MOST = 2
LANES = 128
PIECES = 4
LOG2E = 1.4426950408889634
MESH = pl.DeviceIdType.MESH


def dot(a, b):
    return jnp.dot(a, b, preferred_element_type=jnp.float32)


def row_of_chips(mesh, n):
    where = [tuple(getattr(d, "coords", ())) for d in mesh.devices.reshape(n, -1)[:, 0]]
    if len(where[0]) != 3:
        return 1
    last = [k for k in range(n) if where[k][2] == where[0][2]]
    wide = len(last) // 2
    even = last == list(range(len(last))) and wide > 0 and n % (2 * wide) == 0
    return wide if even else 1


def kernel(
    n,
    n_tp,
    wide,
    x_hbm,
    wq_hbm,
    wk_hbm,
    wv_hbm,
    wo_hbm,
    scale_hbm,
    hot_hbm,
    chosen_hbm,
    out,
    x,
    wq,
    wk,
    wv,
    wo,
    q,
    local,
    pool,
    kvg,
    heads,
    sent,
    got,
    mine_part,
    bias,
    scale_ref,
    hot_ref,
    chosen_ref,
    slot_ref,
    small_sem,
    load_sem,
    wo_sem,
    pass_send,
    hot_recv,
    part_recv,
    ready,
    ready_tp,
):
    me = lax.axis_index("kv")
    t = lax.axis_index("tp")
    own = local.shape[0]
    width = local.shape[2]
    nsel = chosen_ref.shape[1]
    nhot = hot_ref.shape[0]
    blocks = chosen_ref.shape[0]
    head_count = scale_ref.shape[0]
    kv_heads = wk.shape[1] // HD
    pairs = head_count // kv_heads // 2
    keys = nsel * KB
    part_cols = wo.shape[2]
    partner = me + 1 - 2 * lax.rem(me, 2)
    half = n // 2

    depth = x.shape[1] // PIECES
    cuts = [slice(i * depth, (i + 1) * depth) for i in range(PIECES)]
    loads = [
        [
            pltpu.make_async_copy(x_hbm.at[:, cut], x.at[:, cut], load_sem.at[3 * i]),
            pltpu.make_async_copy(wk_hbm.at[cut], wk.at[cut], load_sem.at[3 * i + 1]),
            pltpu.make_async_copy(wv_hbm.at[cut], wv.at[cut], load_sem.at[3 * i + 2]),
        ]
        for i, cut in enumerate(cuts)
    ]
    smalls = [
        pltpu.make_async_copy(hot_hbm, hot_ref, small_sem.at[0]),
        pltpu.make_async_copy(chosen_hbm, chosen_ref, small_sem.at[1]),
        pltpu.make_async_copy(scale_hbm, scale_ref, small_sem.at[2]),
    ]
    for load in loads[0]:
        load.start()
    for small in smalls:
        small.start()
    for piece in loads[1:]:
        for load in piece:
            load.start()
    q_chunk = wq.shape[2]
    wq_loads = [
        pltpu.make_async_copy(wq_hbm.at[:, pl.ds(i * q_chunk, q_chunk)], wq.at[i], small_sem.at[i])
        for i in range(wq.shape[0])
    ]
    targets = [lax.rem(t + k, n_tp) for k in range(n_tp)]
    order = list(range(1, n_tp)) + [0]
    wo_loads = [
        pltpu.make_async_copy(
            wo_hbm.at[:, pl.ds(pl.multiple_of(targets[k] * part_cols, LANES), part_cols)],
            wo.at[k],
            wo_sem.at[k],
        )
        for k in range(n_tp)
    ]

    barrier = pltpu.get_barrier_semaphore()

    rank = lax.div(me, 2)
    core = lax.rem(me, 2)
    level = lax.div(rank, wide)
    place = lax.rem(rank, wide)
    top = half // wide - 1
    below = jnp.where(level == top, rank, level + place)

    def across(chip):
        return (2 * chip + 1 - core, t)

    def direct(low, high):
        high_level = lax.div(high, wide)
        return (
            (high_level == top)
            | (high_level == lax.div(low, wide))
            | (lax.rem(high, wide) == lax.rem(low, wide))
        )

    def greet(j, carry):
        @pl.when(direct(rank, rank + j))
        def _():
            pl.semaphore_signal(
                barrier, inc=1, device_id=across(rank + j), device_id_type=MESH
            )

        return carry

    lax.fori_loop(1, half - rank, greet, 0)

    @pl.when(core == 1)
    def _():
        pl.semaphore_signal(barrier, inc=1, device_id=(partner, t), device_id_type=MESH)

    for k in range(1, n_tp):

        @pl.when(targets[k] > t)
        def _(other=targets[k]):
            pl.semaphore_signal(barrier, inc=1, device_id=(me, other), device_id_type=MESH)


    def tell(j, carry):
        @pl.when(direct(rank - j, rank))
        def _():
            pl.semaphore_signal(
                ready.at[j], inc=1, device_id=across(rank - j), device_id_type=MESH
            )

        return carry

    def meet():
        expected = below + 1 - core + t
        pl.when(expected > 0)(lambda: pl.semaphore_wait(barrier, expected))
        lax.fori_loop(1, rank + 1, tell, 0)

        @pl.when(core == 0)
        def _():
            pl.semaphore_signal(
                ready.at[0], inc=1, device_id=(partner, t), device_id_type=MESH
            )

        for k in range(1, n_tp):

            @pl.when(targets[k] < t)
            def _(other=targets[k]):
                pl.semaphore_signal(
                    ready_tp.at[t - 1], inc=1, device_id=(me, other), device_id_type=MESH
                )


    pl.when(rank > 0)(meet)
    for small in smalls:
        small.wait()
    hots = [hot_ref[h] for h in range(nhot)]
    owners = [lax.div(hot, own) for hot in hots]
    mine = [jnp.int32(0), jnp.int32(0)]
    for h in range(nhot):
        turn = jnp.int32(0)
        for g in range(h):
            turn = turn + (owners[g] == owners[h]).astype(jnp.int32)
        slot_ref[h] = jnp.where(lax.div(owners[h], 2) > rank, 0, own + owners[h] * HOT_MOST + turn)
        offset = hots[h] - owners[h] * own
        for r in range(HOT_MOST):
            mine[r] = jnp.where((owners[h] == me) & (turn == r), offset, mine[r])

    total = None
    middle = x.shape[0] // 2
    for piece, cut in zip(loads, cuts):
        for load in piece:
            load.wait()
        if piece is loads[0]:
            for load in wq_loads:
                load.start()
            for k in order:
                wo_loads[k].start()
        both = jnp.concatenate([wk[cut], wv[cut]], axis=1)
        term = [dot(x[:middle, cut], both), dot(x[middle:, cut], both)]
        total = term if total is None else [a + b for a, b in zip(total, term)]
    packed = jnp.concatenate(total, axis=0).astype(jnp.bfloat16).reshape(own, KB, width)
    local[...] = packed
    pool[pl.ds(0, own)] = packed
    first = own + me * HOT_MOST
    for r in range(HOT_MOST):
        pool[first + r] = local[mine[r]]

    def give(source, device, send):
        rows = pl.ds(own + source * HOT_MOST, HOT_MOST)
        return pltpu.make_async_remote_copy(
            src_ref=pool.at[rows],
            dst_ref=pool.at[rows],
            send_sem=send,
            recv_sem=hot_recv.at[source],
            device_id=(device, t),
            device_id_type=MESH,
        )

    pl.when(rank == 0)(meet)
    pl.when(core == 1)(lambda: pl.semaphore_wait(ready.at[0], 1))
    give(me, partner, load_sem.at[0]).start()

    def send_own(j, carry):
        @pl.when(direct(rank, rank + j))
        def _():
            pl.semaphore_wait(ready.at[j], 1)
            give(me, across(rank + j)[0], load_sem.at[j]).start()

        return carry

    first = jnp.where(level == 0, jnp.maximum(top * wide - rank, 1), half - rank)
    lax.fori_loop(1, first, send_own, 0)

    lane = lax.broadcasted_iota(jnp.int32, (1, keys), 1)
    in_block = lax.rem(lane, KB)
    entry_of = lax.div(lane, KB)

    def mask(b, carry):
        key_pos = in_block
        for e in range(nsel):
            code = chosen_ref[b, e]
            listed = jnp.clip(code - own, 0, nhot - 1)
            block_id = jnp.where(code < own, me * own + code, hot_ref[listed])
            key_pos = jnp.where(entry_of == e, block_id * KB + in_block, key_pos)
        query_pos = (me * blocks + b) * QB + lax.broadcasted_iota(jnp.int32, (QB, keys), 0)
        bias[b] = jnp.where(key_pos <= query_pos, 0.0, -jnp.inf).astype(jnp.float32)
        return carry

    lax.fori_loop(0, blocks, mask, 0)

    def relay(j, m):
        mate = level * wide + lax.rem(place + m, wide)
        return give(across(rank - j * wide)[0], 2 * mate + core, load_sem.at[half + (j - 1) * (wide - 1) + m - 1])

    def pass_on(j):
        copy = give(across(rank - j)[0], partner, pass_send.at[j - 1])
        copy.wait_recv()
        copy.start()

    def pass_column(j, carry):
        pass_on(j * wide)
        for m in range(1, wide):
            relay(j, m).start()
        return carry

    def pass_rest(j, carry):
        pl.when((level == top) | (lax.rem(j, wide) != 0))(lambda: pass_on(j))
        return carry

    columns = jnp.where(level == top, 0, level)
    lax.fori_loop(1, columns + 1, pass_column, 0)
    for i in range(wq.shape[0]):
        wq_loads[i].wait()
        q[:, i * q_chunk : (i + 1) * q_chunk] = dot(x[...], wq[i]).astype(jnp.bfloat16)
        if i == 0:
            lax.fori_loop(first, half - rank, send_own, 0)
    lax.fori_loop(1, rank + 1, pass_rest, 0)

    def land(j, carry):
        give(2 * (rank - j) + core, partner, pass_send.at[0]).wait_recv()
        return carry

    give(partner, partner, pass_send.at[0]).wait_recv()
    lax.fori_loop(1, rank + 1, land, 0)
    for k in range(1, n_tp):
        wo_loads[k].wait()

    low = lax.broadcasted_iota(jnp.int32, (keys, LANES), 1) < HD
    zero = jnp.zeros((keys, LANES), jnp.bfloat16)
    ones = jnp.ones((keys, LANES), jnp.bfloat16)
    ones_low, ones_high = jnp.where(low, ones, zero), jnp.where(low, zero, ones)

    give(me, partner, load_sem.at[0]).wait_send()

    def drain_hot(j, carry):
        @pl.when(direct(rank, rank + j))
        def _():
            give(me, partner, load_sem.at[j]).wait_send()

        return carry

    lax.fori_loop(1, half - rank, drain_hot, 0)

    def drain_relay(j, carry):
        for m in range(1, wide):
            relay(j, m).wait_send()
        return carry

    lax.fori_loop(1, columns + 1, drain_relay, 0)

    steps = sent.shape[1]
    for k in range(1, n_tp):

        @pl.when(targets[k] > t)
        def _(other=targets[k]):
            pl.semaphore_wait(ready_tp.at[other - 1], 1)


    def part_copy(k, b):
        at = (k - 1) * steps + b
        return pltpu.make_async_remote_copy(
            src_ref=sent.at[k - 1, b],
            dst_ref=got.at[k - 1, b],
            send_sem=load_sem.at[at],
            recv_sem=part_recv.at[at],
            device_id=(me, targets[k]),
            device_id_type=MESH,
        )

    def attend(step, carry):
        b = lax.div(step, QB // QR)
        half_rows = pl.ds(pl.multiple_of(lax.rem(step, QB // QR) * QR, QR), QR)
        lift = bias[b, half_rows, :]
        for e in range(nsel):
            code = chosen_ref[b, e]
            listed = jnp.clip(code - own, 0, nhot - 1)
            row = jnp.where(code < own, code, slot_ref[listed])
            kvg[e * KB : (e + 1) * KB, :] = pool[row]
        rows = pl.ds(pl.multiple_of(step * QR, QR), QR)

        def spread(u):
            tile = kvg[:, (u // 2) * LANES : (u // 2 + 1) * LANES]
            turned = jnp.concatenate([tile[:, HD:], tile[:, :HD]], axis=1)
            if u % 2 == 1:
                tile, turned = turned, tile
            return jnp.where(low, tile, zero), jnp.where(low, zero, turned)

        for c in range(kv_heads):
            k_low, k_high = spread(c)
            k_both = jnp.concatenate([k_low, k_high], axis=0)
            v_low, v_high = spread(kv_heads + c)
            v_parts = [
                jnp.concatenate([v_low, ones_low], axis=1),
                jnp.concatenate([v_high, ones_high], axis=1),
            ]
            first_pair = c * pairs
            q_rows = jnp.concatenate(
                [
                    q[rows, (first_pair + p) * LANES : (first_pair + p + 1) * LANES]
                    for p in range(pairs)
                ],
                axis=0,
            )
            scores = lax.dot_general(
                q_rows, k_both, (((1,), (1,)), ((), ())), preferred_element_type=jnp.float32
            )
            lifted = []
            for p in range(pairs):
                both = []
                for s in range(2):
                    factor = scale_ref[(first_pair + p) * 2 + s] * (HD**-0.5 * LOG2E)
                    part = scores[p * QR : (p + 1) * QR, s * keys : (s + 1) * keys]
                    part = part * factor + lift
                    top = jnp.max(part, axis=1, keepdims=True)
                    both.append(jnp.exp2(part - top).astype(jnp.bfloat16))
                lifted.append(both)
            summed = sum(
                dot(jnp.concatenate([pair[s] for pair in lifted], axis=0), v_parts[s])
                for s in range(2)
            )
            held = (summed[:, :LANES] / summed[:, LANES:]).astype(jnp.bfloat16)
            for p in range(pairs):
                heads[rows, (first_pair + p) * LANES : (first_pair + p + 1) * LANES] = held[
                    p * QR : (p + 1) * QR
                ]
        for k in range(1, n_tp):
            sent[k - 1, step] = dot(heads[rows, :], wo[k]).astype(jnp.bfloat16)
            part_copy(k, step).start()
        return carry

    lax.fori_loop(0, steps, attend, 0)

    wo_loads[0].wait()
    mine_part[...] = dot(heads[...], wo[0]).astype(jnp.bfloat16)

    def drain_pass(j, carry):
        give(me, partner, pass_send.at[j - 1]).wait_send()
        return carry

    lax.fori_loop(1, rank + 1, drain_pass, 0)

    def finish(b, carry):
        rows = pl.ds(pl.multiple_of(b * QR, QR), QR)
        total = mine_part[rows, :].astype(jnp.float32)
        for k in range(1, n_tp):
            part_copy(k, b).wait()
            total = total + got[k - 1, b].astype(jnp.float32)
        out[rows, :] = total.astype(jnp.bfloat16)
        return carry

    lax.fori_loop(0, steps, finish, 0)


def solution(mesh):
    n, n_tp = mesh.shape["kv"], mesh.shape["tp"]
    wide = row_of_chips(mesh, n)

    def local(x, wq, wk, wv, wo, scale, hot, chosen):
        tok, depth = x.shape
        own = tok // KB
        width = wk.shape[1] + wv.shape[1]
        blocks, nsel = chosen.shape
        q_cols = wq.shape[1]
        q_chunk = 512
        part_cols = wo.shape[1] // n_tp
        bf16 = jnp.bfloat16
        relays = (n // 2 // wide - 1) * (wide - 1)
        shared = max(3 * PIECES, n // 2 + relays, (n_tp - 1) * (tok // QR))
        dma = pltpu.SemaphoreType.DMA
        any_space = pl.BlockSpec(memory_space=pl.ANY)
        vmem = pl.BlockSpec(memory_space=pltpu.VMEM)
        return pl.pallas_call(
            functools.partial(kernel, n, n_tp, wide),
            out_shape=pltpu.VMEM((tok, part_cols), bf16),
            in_specs=[any_space] * 8,
            out_specs=vmem,
            scratch_shapes=[
                pltpu.VMEM((tok, depth), bf16),
                pltpu.VMEM((q_cols // q_chunk, depth, q_chunk), bf16),
                pltpu.VMEM(wk.shape, bf16),
                pltpu.VMEM(wv.shape, bf16),
                pltpu.VMEM((n_tp, wo.shape[0], part_cols), bf16),
                pltpu.VMEM((tok, q_cols), bf16),
                pltpu.VMEM((own, KB, width), bf16),
                pltpu.VMEM((own + HOT_MOST * n, KB, width), bf16),
                pltpu.VMEM((nsel * KB, width), bf16),
                pltpu.VMEM((tok, q_cols), bf16),
                pltpu.VMEM((n_tp - 1, tok // QR, QR, part_cols), bf16),
                pltpu.VMEM((n_tp - 1, tok // QR, QR, part_cols), bf16),
                pltpu.VMEM((tok, part_cols), bf16),
                pltpu.VMEM((blocks, QB, nsel * KB), jnp.float32),
                pltpu.SMEM(scale.shape, jnp.float32),
                pltpu.SMEM(hot.shape, jnp.int32),
                pltpu.SMEM(chosen.shape, jnp.int32),
                pltpu.SMEM(hot.shape, jnp.int32),
                dma((max(3, q_cols // q_chunk),)),
                dma((shared,)),
                dma((n_tp,)),
                dma((n // 2 - 1,)),
                dma((n,)),
                dma(((n_tp - 1) * (tok // QR),)),
                pltpu.SemaphoreType.REGULAR((n // 2,)),
                pltpu.SemaphoreType.REGULAR((max(n_tp - 1, 1),)),
            ],
            compiler_params=pltpu.CompilerParams(
                collective_id=0, has_side_effects=True, vmem_limit_bytes=32 * 1024 * 1024
            ),
        )(
            *[
                pltpu.with_memory_space_constraint(a, pltpu.HBM)
                for a in (x, wq, wk, wv, wo, scale, hot, chosen)
            ]
        )

    return jax.shard_map(
        local,
        mesh=mesh,
        in_specs=(
            P("kv", None),
            P(None, "tp"),
            P(None, "tp"),
            P(None, "tp"),
            P("tp", None),
            P("tp"),
            P(),
            P("kv", None),
        ),
        out_specs=P("kv", "tp"),
        check_vma=False,
    )
```

```python
import functools

import jax
import jax.numpy as jnp
from jax import lax
from jax.experimental import pallas as pl
from jax.experimental.pallas import tpu as pltpu
from jax.sharding import PartitionSpec as P

HD = 64
KB = 32
QB = 64
QR = 32
SPAN = 4
HOT_MOST = 2
LANES = 128
PIECES = 4
LOG2E = 1.4426950408889634
MESH = pl.DeviceIdType.MESH


def dot(a, b):
    return jnp.dot(a, b, preferred_element_type=jnp.float32)


def row_of_chips(mesh, n):
    where = [tuple(getattr(d, "coords", ())) for d in mesh.devices.reshape(n, -1)[:, 0]]
    if len(where[0]) != 3:
        return 1
    last = [k for k in range(n) if where[k][2] == where[0][2]]
    wide = len(last) // 2
    even = last == list(range(len(last))) and wide > 0 and n % (2 * wide) == 0
    return wide if even else 1


def kernel(
    n,
    n_tp,
    wide,
    x_hbm,
    wq_hbm,
    wk_hbm,
    wv_hbm,
    wo_hbm,
    scale_hbm,
    hot_hbm,
    chosen_hbm,
    out,
    x,
    wq,
    wk,
    wv,
    wo,
    q,
    local,
    pool,
    kvg,
    heads,
    sent,
    got,
    mine_part,
    bias,
    scale_ref,
    hot_ref,
    chosen_ref,
    slot_ref,
    small_sem,
    load_sem,
    wo_sem,
    pass_send,
    hot_recv,
    part_recv,
    ready,
    ready_tp,
):
    me = lax.axis_index("kv")
    t = lax.axis_index("tp")
    own = local.shape[0]
    width = local.shape[2]
    nsel = chosen_ref.shape[1]
    nhot = hot_ref.shape[0]
    blocks = chosen_ref.shape[0]
    head_count = scale_ref.shape[0]
    kv_heads = wk.shape[1] // HD
    pairs = head_count // kv_heads // 2
    keys = nsel * KB
    part_cols = wo.shape[2]
    partner = me + 1 - 2 * lax.rem(me, 2)
    half = n // 2

    depth = x.shape[1] // PIECES
    cuts = [slice(i * depth, (i + 1) * depth) for i in range(PIECES)]
    loads = [
        [
            pltpu.make_async_copy(x_hbm.at[:, cut], x.at[:, cut], load_sem.at[3 * i]),
            pltpu.make_async_copy(wk_hbm.at[cut], wk.at[cut], load_sem.at[3 * i + 1]),
            pltpu.make_async_copy(wv_hbm.at[cut], wv.at[cut], load_sem.at[3 * i + 2]),
        ]
        for i, cut in enumerate(cuts)
    ]
    smalls = [
        pltpu.make_async_copy(hot_hbm, hot_ref, small_sem.at[0]),
        pltpu.make_async_copy(chosen_hbm, chosen_ref, small_sem.at[1]),
        pltpu.make_async_copy(scale_hbm, scale_ref, small_sem.at[2]),
    ]
    for load in loads[0]:
        load.start()
    for small in smalls:
        small.start()
    for piece in loads[1:]:
        for load in piece:
            load.start()
    q_chunk = wq.shape[2]
    wq_loads = [
        pltpu.make_async_copy(wq_hbm.at[:, pl.ds(i * q_chunk, q_chunk)], wq.at[i], small_sem.at[i])
        for i in range(wq.shape[0])
    ]
    targets = [lax.rem(t + k, n_tp) for k in range(n_tp)]
    order = list(range(1, n_tp)) + [0]
    wo_loads = [
        pltpu.make_async_copy(
            wo_hbm.at[:, pl.ds(pl.multiple_of(targets[k] * part_cols, LANES), part_cols)],
            wo.at[k],
            wo_sem.at[k],
        )
        for k in range(n_tp)
    ]

    barrier = pltpu.get_barrier_semaphore()

    rank = lax.div(me, 2)
    core = lax.rem(me, 2)
    level = lax.div(rank, wide)
    place = lax.rem(rank, wide)
    top = half // wide - 1
    below = jnp.where(level == top, rank, level + place)

    def across(chip):
        return (2 * chip + 1 - core, t)

    def direct(low, high):
        high_level = lax.div(high, wide)
        return (
            (high_level == top)
            | (high_level == lax.div(low, wide))
            | (lax.rem(high, wide) == lax.rem(low, wide))
        )

    def greet(j, carry):
        @pl.when(direct(rank, rank + j))
        def _():
            pl.semaphore_signal(
                barrier, inc=1, device_id=across(rank + j), device_id_type=MESH
            )

        return carry

    lax.fori_loop(1, half - rank, greet, 0)

    @pl.when(core == 1)
    def _():
        pl.semaphore_signal(barrier, inc=1, device_id=(partner, t), device_id_type=MESH)

    for k in range(1, n_tp):

        @pl.when(targets[k] > t)
        def _(other=targets[k]):
            pl.semaphore_signal(barrier, inc=1, device_id=(me, other), device_id_type=MESH)


    def tell(j, carry):
        @pl.when(direct(rank - j, rank))
        def _():
            pl.semaphore_signal(
                ready.at[j], inc=1, device_id=across(rank - j), device_id_type=MESH
            )

        return carry

    def meet():
        expected = below + 1 - core + t
        pl.when(expected > 0)(lambda: pl.semaphore_wait(barrier, expected))
        lax.fori_loop(1, rank + 1, tell, 0)

        @pl.when(core == 0)
        def _():
            pl.semaphore_signal(
                ready.at[0], inc=1, device_id=(partner, t), device_id_type=MESH
            )

        for k in range(1, n_tp):

            @pl.when(targets[k] < t)
            def _(other=targets[k]):
                pl.semaphore_signal(
                    ready_tp.at[t - 1], inc=1, device_id=(me, other), device_id_type=MESH
                )


    pl.when(rank > 0)(meet)
    for small in smalls:
        small.wait()
    hots = [hot_ref[h] for h in range(nhot)]
    owners = [lax.div(hot, own) for hot in hots]
    mine = [jnp.int32(0), jnp.int32(0)]
    for h in range(nhot):
        turn = jnp.int32(0)
        for g in range(h):
            turn = turn + (owners[g] == owners[h]).astype(jnp.int32)
        slot_ref[h] = jnp.where(lax.div(owners[h], 2) > rank, 0, own + owners[h] * HOT_MOST + turn)
        offset = hots[h] - owners[h] * own
        for r in range(HOT_MOST):
            mine[r] = jnp.where((owners[h] == me) & (turn == r), offset, mine[r])

    total = None
    middle = x.shape[0] // 2
    for piece, cut in zip(loads, cuts):
        for load in piece:
            load.wait()
        if piece is loads[0]:
            for load in wq_loads:
                load.start()
            for k in order:
                wo_loads[k].start()
        both = jnp.concatenate([wk[cut], wv[cut]], axis=1)
        term = [dot(x[:middle, cut], both), dot(x[middle:, cut], both)]
        total = term if total is None else [a + b for a, b in zip(total, term)]
    packed = jnp.concatenate(total, axis=0).astype(jnp.bfloat16).reshape(own, KB, width)
    local[...] = packed
    pool[pl.ds(0, own)] = packed
    first = own + me * HOT_MOST
    for r in range(HOT_MOST):
        pool[first + r] = local[mine[r]]

    def give(source, device, send):
        rows = pl.ds(own + source * HOT_MOST, HOT_MOST)
        return pltpu.make_async_remote_copy(
            src_ref=pool.at[rows],
            dst_ref=pool.at[rows],
            send_sem=send,
            recv_sem=hot_recv.at[source],
            device_id=(device, t),
            device_id_type=MESH,
        )

    pl.when(rank == 0)(meet)
    pl.when(core == 1)(lambda: pl.semaphore_wait(ready.at[0], 1))
    give(me, partner, load_sem.at[0]).start()

    def send_own(j, carry):
        @pl.when(direct(rank, rank + j))
        def _():
            pl.semaphore_wait(ready.at[j], 1)
            give(me, across(rank + j)[0], load_sem.at[j]).start()

        return carry

    first = jnp.where(level == 0, jnp.maximum(top * wide - rank, 1), half - rank)
    lax.fori_loop(1, first, send_own, 0)

    lane = lax.broadcasted_iota(jnp.int32, (1, keys), 1)
    in_block = lax.rem(lane, KB)
    entry_of = lax.div(lane, KB)

    def mask(b, carry):
        key_pos = in_block
        for e in range(nsel):
            code = chosen_ref[b, e]
            listed = jnp.clip(code - own, 0, nhot - 1)
            block_id = jnp.where(code < own, me * own + code, hot_ref[listed])
            key_pos = jnp.where(entry_of == e, block_id * KB + in_block, key_pos)
        query_pos = (me * blocks + b) * QB + lax.broadcasted_iota(jnp.int32, (QB, keys), 0)
        bias[b] = jnp.where(key_pos <= query_pos, 0.0, -jnp.inf).astype(jnp.float32)
        return carry

    lax.fori_loop(0, blocks, mask, 0)

    def relay(j, m):
        mate = level * wide + lax.rem(place + m, wide)
        return give(across(rank - j * wide)[0], 2 * mate + core, load_sem.at[half + (j - 1) * (wide - 1) + m - 1])

    def pass_on(j):
        copy = give(across(rank - j)[0], partner, pass_send.at[j - 1])
        copy.wait_recv()
        copy.start()

    def pass_column(j, carry):
        pass_on(j * wide)
        for m in range(1, wide):
            relay(j, m).start()
        return carry

    def pass_rest(j, carry):
        pl.when((level == top) | (lax.rem(j, wide) != 0))(lambda: pass_on(j))
        return carry

    columns = jnp.where(level == top, 0, level)
    lax.fori_loop(1, columns + 1, pass_column, 0)
    for i in range(wq.shape[0]):
        wq_loads[i].wait()
        q[:, i * q_chunk : (i + 1) * q_chunk] = dot(x[...], wq[i]).astype(jnp.bfloat16)
        if i == 0:
            lax.fori_loop(first, half - rank, send_own, 0)
    lax.fori_loop(1, rank + 1, pass_rest, 0)

    def land(j, carry):
        give(2 * (rank - j) + core, partner, pass_send.at[0]).wait_recv()
        return carry

    give(partner, partner, pass_send.at[0]).wait_recv()
    lax.fori_loop(1, rank + 1, land, 0)
    for k in range(1, n_tp):
        wo_loads[k].wait()

    low = lax.broadcasted_iota(jnp.int32, (keys, LANES), 1) < HD
    zero = jnp.zeros((keys, LANES), jnp.bfloat16)
    ones = jnp.ones((keys, LANES), jnp.bfloat16)
    ones_low, ones_high = jnp.where(low, ones, zero), jnp.where(low, zero, ones)

    give(me, partner, load_sem.at[0]).wait_send()

    def drain_hot(j, carry):
        @pl.when(direct(rank, rank + j))
        def _():
            give(me, partner, load_sem.at[j]).wait_send()

        return carry

    lax.fori_loop(1, half - rank, drain_hot, 0)

    def drain_relay(j, carry):
        for m in range(1, wide):
            relay(j, m).wait_send()
        return carry

    lax.fori_loop(1, columns + 1, drain_relay, 0)

    steps = sent.shape[1]
    for k in range(1, n_tp):

        @pl.when(targets[k] > t)
        def _(other=targets[k]):
            pl.semaphore_wait(ready_tp.at[other - 1], 1)


    bundles = (steps - 1) // SPAN
    bundled = bundles * SPAN
    marks = bundles + steps - bundled

    def part_copy(k, b, count=1):
        at = (k - 1) * steps + b
        mark = jnp.where(b < bundled, lax.div(b, SPAN), b - bundled + bundles)
        return pltpu.make_async_remote_copy(
            src_ref=sent.at[k - 1, pl.ds(b, count)],
            dst_ref=got.at[k - 1, pl.ds(b, count)],
            send_sem=load_sem.at[at],
            recv_sem=part_recv.at[(k - 1) * marks + mark],
            device_id=(me, targets[k]),
            device_id_type=MESH,
        )

    def attend(step, carry):
        b = lax.div(step, QB // QR)
        half_rows = pl.ds(pl.multiple_of(lax.rem(step, QB // QR) * QR, QR), QR)
        lift = bias[b, half_rows, :]
        for e in range(nsel):
            code = chosen_ref[b, e]
            listed = jnp.clip(code - own, 0, nhot - 1)
            row = jnp.where(code < own, code, slot_ref[listed])
            kvg[e * KB : (e + 1) * KB, :] = pool[row]
        rows = pl.ds(pl.multiple_of(step * QR, QR), QR)

        def spread(u):
            tile = kvg[:, (u // 2) * LANES : (u // 2 + 1) * LANES]
            turned = jnp.concatenate([tile[:, HD:], tile[:, :HD]], axis=1)
            if u % 2 == 1:
                tile, turned = turned, tile
            return jnp.where(low, tile, zero), jnp.where(low, zero, turned)

        for c in range(kv_heads):
            k_low, k_high = spread(c)
            k_both = jnp.concatenate([k_low, k_high], axis=0)
            v_low, v_high = spread(kv_heads + c)
            v_parts = [
                jnp.concatenate([v_low, ones_low], axis=1),
                jnp.concatenate([v_high, ones_high], axis=1),
            ]
            first_pair = c * pairs
            q_rows = jnp.concatenate(
                [
                    q[rows, (first_pair + p) * LANES : (first_pair + p + 1) * LANES]
                    for p in range(pairs)
                ],
                axis=0,
            )
            scores = lax.dot_general(
                q_rows, k_both, (((1,), (1,)), ((), ())), preferred_element_type=jnp.float32
            )
            lifted = []
            for p in range(pairs):
                both = []
                for s in range(2):
                    factor = scale_ref[(first_pair + p) * 2 + s] * (HD**-0.5 * LOG2E)
                    part = scores[p * QR : (p + 1) * QR, s * keys : (s + 1) * keys]
                    part = part * factor + lift
                    top = jnp.max(part, axis=1, keepdims=True)
                    both.append(jnp.exp2(part - top).astype(jnp.bfloat16))
                lifted.append(both)
            summed = sum(
                dot(jnp.concatenate([pair[s] for pair in lifted], axis=0), v_parts[s])
                for s in range(2)
            )
            held = (summed[:, :LANES] / summed[:, LANES:]).astype(jnp.bfloat16)
            for p in range(pairs):
                heads[rows, (first_pair + p) * LANES : (first_pair + p + 1) * LANES] = held[
                    p * QR : (p + 1) * QR
                ]
        for k in range(1, n_tp):
            sent[k - 1, step] = dot(heads[rows, :], wo[k]).astype(jnp.bfloat16)
            part_copy(k, step).start()
        return carry

    lax.fori_loop(0, steps, attend, 0)

    wo_loads[0].wait()
    mine_part[...] = dot(heads[...], wo[0]).astype(jnp.bfloat16)

    def drain_pass(j, carry):
        give(me, partner, pass_send.at[j - 1]).wait_send()
        return carry

    lax.fori_loop(1, rank + 1, drain_pass, 0)

    def drain_part(b, carry):
        for k in range(1, n_tp):
            part_copy(k, b).wait_send()
        return carry

    def finish(b):
        rows = pl.ds(pl.multiple_of(b * QR, QR), QR)
        total = mine_part[rows, :].astype(jnp.float32)
        for k in range(1, n_tp):
            total = total + got[k - 1, b].astype(jnp.float32)
        out[rows, :] = total.astype(jnp.bfloat16)

    def finish_bundle(g, carry):
        for k in range(1, n_tp):
            part_copy(k, g * SPAN, SPAN).wait_recv()
        for r in range(SPAN):
            finish(g * SPAN + r)
        return carry

    def finish_one(b, carry):
        for k in range(1, n_tp):
            part_copy(k, b).wait_recv()
        finish(b)
        return carry

    lax.fori_loop(0, bundles, finish_bundle, 0)
    lax.fori_loop(bundled, steps, finish_one, 0)
    lax.fori_loop(0, steps, drain_part, 0)


def solution(mesh):
    n, n_tp = mesh.shape["kv"], mesh.shape["tp"]
    wide = row_of_chips(mesh, n)

    def local(x, wq, wk, wv, wo, scale, hot, chosen):
        tok, depth = x.shape
        own = tok // KB
        width = wk.shape[1] + wv.shape[1]
        blocks, nsel = chosen.shape
        q_cols = wq.shape[1]
        q_chunk = 512
        part_cols = wo.shape[1] // n_tp
        bf16 = jnp.bfloat16
        steps = tok // QR
        marks = (steps - 1) // SPAN + steps - (steps - 1) // SPAN * SPAN
        relays = (n // 2 // wide - 1) * (wide - 1)
        shared = max(3 * PIECES, n // 2 + relays, (n_tp - 1) * (tok // QR))
        dma = pltpu.SemaphoreType.DMA
        any_space = pl.BlockSpec(memory_space=pl.ANY)
        vmem = pl.BlockSpec(memory_space=pltpu.VMEM)
        return pl.pallas_call(
            functools.partial(kernel, n, n_tp, wide),
            out_shape=pltpu.VMEM((tok, part_cols), bf16),
            in_specs=[any_space] * 8,
            out_specs=vmem,
            scratch_shapes=[
                pltpu.VMEM((tok, depth), bf16),
                pltpu.VMEM((q_cols // q_chunk, depth, q_chunk), bf16),
                pltpu.VMEM(wk.shape, bf16),
                pltpu.VMEM(wv.shape, bf16),
                pltpu.VMEM((n_tp, wo.shape[0], part_cols), bf16),
                pltpu.VMEM((tok, q_cols), bf16),
                pltpu.VMEM((own, KB, width), bf16),
                pltpu.VMEM((own + HOT_MOST * n, KB, width), bf16),
                pltpu.VMEM((nsel * KB, width), bf16),
                pltpu.VMEM((tok, q_cols), bf16),
                pltpu.VMEM((n_tp - 1, tok // QR, QR, part_cols), bf16),
                pltpu.VMEM((n_tp - 1, tok // QR, QR, part_cols), bf16),
                pltpu.VMEM((tok, part_cols), bf16),
                pltpu.VMEM((blocks, QB, nsel * KB), jnp.float32),
                pltpu.SMEM(scale.shape, jnp.float32),
                pltpu.SMEM(hot.shape, jnp.int32),
                pltpu.SMEM(chosen.shape, jnp.int32),
                pltpu.SMEM(hot.shape, jnp.int32),
                dma((max(3, q_cols // q_chunk),)),
                dma((shared,)),
                dma((n_tp,)),
                dma((n // 2 - 1,)),
                dma((n,)),
                dma(((n_tp - 1) * marks,)),
                pltpu.SemaphoreType.REGULAR((n // 2,)),
                pltpu.SemaphoreType.REGULAR((max(n_tp - 1, 1),)),
            ],
            compiler_params=pltpu.CompilerParams(
                collective_id=0, has_side_effects=True, vmem_limit_bytes=32 * 1024 * 1024
            ),
        )(
            *[
                pltpu.with_memory_space_constraint(a, pltpu.HBM)
                for a in (x, wq, wk, wv, wo, scale, hot, chosen)
            ]
        )

    return jax.shard_map(
        local,
        mesh=mesh,
        in_specs=(
            P("kv", None),
            P(None, "tp"),
            P(None, "tp"),
            P(None, "tp"),
            P("tp", None),
            P("tp"),
            P(),
            P("kv", None),
        ),
        out_specs=P("kv", "tp"),
        check_vma=False,
    )
```
